32 devices in a mesh: ep: 8 (over z, x), tp: 4 (over y, core).
Axes of the slice: x: 2, y: 2, z: 4, core: 2. Of those that a mesh axis runs over, the one named last changes fastest.
Arguments:
- receptance: bfloat16 [4096, 1024], P('ep', 'tp'), may hold values from -6 to 6
- key_matrix: bfloat16 [4096, 1024], P('ep', 'tp'), may hold values from -6 to 6
- value_matrix: bfloat16 [4096, 1024], P('ep', 'tp'), may hold values from -6 to 6
- decay_data_term: bfloat16 [4096, 1024], P('ep', 'tp'), may hold values from -3.5 to 3.5
- correction_rate_data: bfloat16 [4096, 1024], P('ep', 'tp'), may hold values from -6 to 6
- output_gate_input: bfloat16 [4096, 1024], P('ep', 'tp'), may hold values from -6 to 6
- decay_channel_offset: float32 [1024], P('tp'), may hold values from -12 to -2
- correction_rate_offset: float32 [1024], P('tp'), may hold values from -12 to 1
- extra_head_log_decay: float32 [4096, 16], P('ep', 'tp'), may hold values from -2.1 to 0, as said below
- head_norm_gain: float32 [1024], P('tp'), may hold values from 0.1 to 1.9
- mixer_output_weight: bfloat16 [1024, 2048], P('tp'), may hold values from -0.1875 to 0.1875
- expert_layer_input: bfloat16 [1024, 2048], P('ep'), may hold values from -6 to 6
- feedforward_norm_gain: float32 [2048], replicated, may hold values from 0.1 to 1.9
- group_router_weight: bfloat16 [2048, 4], replicated, may hold values from -0.125 to 0.125
- expert_router_weight: bfloat16 [2048, 8], replicated, may hold values from -0.125 to 0.125
- routes: int32 [1024, 2], P('ep'), may hold values from 0 to 7, all different within a row; in each aligned block of 128 rows (0 to 127, 128 to 255, ...) at most 64 rows name the same one
- expert_gate_weight: bfloat16 [8, 2048, 4096], P('ep', None, 'tp'), may hold values from -0.125 to 0.125
- expert_up_weight: bfloat16 [8, 2048, 4096], P('ep', None, 'tp'), may hold values from -0.125 to 0.125
- expert_down_weight: bfloat16 [8, 4096, 2048], P('ep', 'tp'), may hold values from -0.09375 to 0.09375
Outputs:
- token_mixer_output: bfloat16 [4096, 2048], P(('ep', 'tp'))
- expert_out: bfloat16 [1024, 2048], P('ep', 'tp')
The draws below stay inside these ranges and needn't reach their ends.
Inputs may be any that keep to these rules, and one draw needn't show every extreme that they name: A token's routes are distinct. Within the rows of one index of ep, no expert is named by more than 64 rows, a bound that some block reaches. `extra_head_log_decay`: entries are zero or negative; each head has a few nonzero positions.
All inputs are finite; a program needn't handle non-finite values.
Results may differ from the reference program's by a relative error of at most 0.022.
Values may be sent and summed in bfloat16 or wider, within the bound.
No kernel may reach another device: no remote copies, remote signals or barrier semaphores. Data moves between devices by JAX's collectives and lax.ppermute only.
A program may use at most 128 MiB of HBM per device.

```python
import math
import jax
import jax.numpy as jnp
import numpy as np
from jax import lax

D = 2048
HEAD_DIM = 64
HEADS = 16
MIX = 1024
FF = 4096
GROUPS = 4
EXPERTS = 8
TOP = 2
MIX_ROWS = 512
MIX_TOKENS = 4096
MOE_ROWS = 128
MOE_TOKENS = 1024
CAP = 64
N_EP = 8
N_TP = 4


def slow_heads(key):
    share = 0.5
    return jax.random.uniform(jax.random.fold_in(key, 101), (HEADS,)) < share


def draw_decay_channel_offset(key, part):
    slow = slow_heads(key)
    slow_level = math.log(0.5 / MIX_TOKENS) + 0.5
    fast_level = math.log(0.03) + 0.5
    level = jnp.where(slow, slow_level, fast_level)
    jitter = jax.random.uniform(jax.random.fold_in(key, 3), (HEADS, HEAD_DIM), jnp.float32, -0.3, 0.3)
    return (level[:, None] + jitter).reshape(MIX).astype(jnp.float32)


def draw_correction_rate_offset(key, part):
    slow = slow_heads(key)
    slow_level = math.log(6.0 / MIX_TOKENS)
    spread = jax.random.uniform(jax.random.fold_in(key, 5), (HEADS, HEAD_DIM), jnp.float32, -1.0, 1.0)
    level = jnp.where(slow[:, None], slow_level + 0.3 * spread, spread)
    return level.reshape(MIX).astype(jnp.float32)


def draw_decay_data_term(key, part):
    blocks = MIX_TOKENS // MIX_ROWS
    offset = jax.random.uniform(jax.random.fold_in(key, 7), (blocks, 1, HEADS, 1), jnp.float32, -0.4, 0.4)
    noise = 0.5 * jax.random.normal(jax.random.fold_in(key, 9), (blocks, MIX_ROWS, HEADS, HEAD_DIM), jnp.float32)
    return (offset + noise).reshape(MIX_TOKENS, MIX).astype(jnp.bfloat16)


def draw_extra_head_log_decay(key, part):
    where_at = jax.random.randint(jax.random.fold_in(key, 13), (3, HEADS), 0, MIX_TOKENS)
    depth = jnp.log(jax.random.uniform(jax.random.fold_in(key, 17), (3, HEADS), jnp.float32, 0.5, 0.8))
    positions = jnp.arange(MIX_TOKENS)[:, None, None]
    struck = positions == where_at[None, :, :]
    return jnp.sum(jnp.where(struck, depth[None, :, :], 0.0), axis=1).astype(jnp.float32)


def levels(rng, extent, shards, low, high):
    loudness, own = 1.0, jax.random.fold_in(rng, 6)
    for position, blocks in shards:
        draws = jnp.exp(jax.random.uniform(jax.random.fold_in(own, position), (blocks,), jnp.float32, low / len(shards), high / len(shards)))
        loudness = loudness * jnp.repeat(draws, extent[position] // blocks).reshape([-1 if axis == position else 1 for axis in range(len(extent))])
    return loudness


def routed_block(own_key, own, number, rows, count, top, reach, skew):
    sequence = jax.random.permutation(own_key, count)
    heavy_load, ordinary = shares(count, rows * top, reach, skew, True), shares(count, rows * top, reach, skew, False)
    places = jnp.arange(count)

    def named(tallies, offset_by):
        used = int((tallies > 0).sum())
        fixed = max(1, used // 4)
        shifted = fixed + (places - fixed + offset_by * (used - fixed)) % max(1, count - fixed)
        return jnp.zeros((count,), jnp.int32).at[sequence[jnp.where(places < fixed, places, shifted)]].set(jnp.asarray(tallies, jnp.int32))

    tallies = jnp.where(number % 4 == 0, named(heavy_load, number // 4), named(ordinary, number - number // 4 - 1))
    mixed = jax.random.permutation(jax.random.fold_in(own, 3), count)
    giver, sink = mixed[0:count // 2 * 2:2], mixed[1:count // 2 * 2:2]
    margin = jnp.minimum(tallies[giver] - 1, reach - tallies[sink]) // 2
    margin = jnp.where((giver == sequence[0]) | (sink == sequence[0]) | (tallies[sink] == 0), 0, jnp.maximum(margin, 0))
    shifted = jax.random.randint(jax.random.fold_in(own, 4), (count // 2,), 0, 1 << 20) % (margin + 1)
    tallies = tallies.at[giver].add(-shifted).at[sink].add(shifted)
    labels = jnp.searchsorted(jnp.cumsum(tallies), jnp.arange(rows * top), side="right").astype(jnp.int32)
    table = labels.reshape(top, rows).T
    table = table[jax.random.permutation(jax.random.fold_in(own, 1), rows)]
    offset_by = jax.random.randint(jax.random.fold_in(own, 2), (rows, 1), 0, top)
    return jnp.take_along_axis(table, (jnp.arange(top)[None, :] + offset_by) % top, axis=1)


def shares(amount, total, bound, lean, full):
    portions = [(1 << 20) // math.isqrt(standing ** lean) + 1 for standing in range(1, amount + 1)]
    largest = bound if full else min(bound, max(-(-total // amount), total * portions[0] // sum(portions)))
    least = 1 if total - largest >= amount - 1 else 0
    counts, surplus = [largest] + [least] * (amount - 1), total - largest - least * (amount - 1)
    while surplus > 0:
        movable = [i for i in range(1, amount) if counts[i] < largest] or [i for i in range(1, amount) if counts[i] < bound]
        pool, remaining = sum([portions[i] for i in movable]), surplus
        for i in movable:
            addition = min(bound - counts[i], max(1, remaining * portions[i] // pool), surplus)
            counts[i] = counts[i] + addition
            surplus = surplus - addition
    return np.array(counts)


def centred(key, shape, scale, reach, pieces=(), held_as=jnp.bfloat16):
    drawn = scale * jax.random.normal(key, shape, jnp.float32)
    if pieces:
        drawn = drawn * levels(key, shape, pieces, -0.22, 0.18)
    return jnp.clip(drawn, -reach, reach).astype(held_as)


def setup_inputs(seed: int = 0) -> dict:
    splits = jax.random.split(jax.random.key(seed), 20)
    receptance = centred(splits[0], (MIX_TOKENS, MIX), 1.0, 6.0, ((0, 8), (1, 4)))
    key_matrix = centred(splits[1], (MIX_TOKENS, MIX), 1.0, 6.0, ((0, 8), (1, 4)))
    value_matrix = centred(splits[2], (MIX_TOKENS, MIX), 1.0, 6.0, ((0, 8), (1, 4)))
    decay_data_term = draw_decay_data_term(jax.random.fold_in(splits[19], 71), 0)
    correction_rate_data = centred(splits[4], (MIX_TOKENS, MIX), 1.0, 6.0, ((0, 8), (1, 4)))
    output_gate_input = centred(splits[5], (MIX_TOKENS, MIX), 1.0, 6.0, ((0, 8), (1, 4)))
    decay_channel_offset = draw_decay_channel_offset(jax.random.fold_in(splits[19], 71), 0)
    correction_rate_offset = draw_correction_rate_offset(jax.random.fold_in(splits[19], 71), 0)
    extra_head_log_decay = draw_extra_head_log_decay(jax.random.fold_in(splits[19], 71), 0)
    head_norm_gain = jnp.clip(1.0 + 0.18 * jax.random.normal(splits[9], (MIX,), jnp.float32), 0.1, 1.9)
    mixer_output_weight = centred(splits[10], (MIX, D), MIX ** -0.5, 0.1875, ((0, 4),))
    expert_layer_input = centred(splits[11], (MOE_TOKENS, D), 1.0, 6.0, ((0, 8),))
    feedforward_norm_gain = jnp.clip(1.0 + 0.18 * jax.random.normal(splits[12], (D,), jnp.float32), 0.1, 1.9)
    group_router_weight = centred(splits[13], (D, GROUPS), D ** -0.5, 0.125)
    expert_router_weight = centred(splits[14], (D, EXPERTS), D ** -0.5, 0.125)
    routes_keys = jax.random.split(jax.random.fold_in(splits[15], 1), MOE_TOKENS // MOE_ROWS)
    routes_turns = jax.random.permutation(jax.random.fold_in(splits[15], 3), MOE_TOKENS // MOE_ROWS)
    routes = jax.vmap(lambda own, number: routed_block(jax.random.fold_in(splits[15], 2), own, number, MOE_ROWS, EXPERTS, TOP, CAP, 2))(routes_keys, routes_turns).reshape((MOE_TOKENS, TOP))
    expert_gate_weight = centred(splits[16], (EXPERTS, D, FF), D ** -0.5, 0.125, ((0, 8), (2, 4)))
    expert_up_weight = centred(splits[17], (EXPERTS, D, FF), D ** -0.5, 0.125, ((0, 8), (2, 4)))
    expert_down_weight = centred(splits[18], (EXPERTS, FF, D), FF ** -0.5, 0.09375, ((0, 8), (1, 4)))
    return {"receptance": receptance, "key_matrix": key_matrix, "value_matrix": value_matrix, "decay_data_term": decay_data_term, "correction_rate_data": correction_rate_data, "output_gate_input": output_gate_input, "decay_channel_offset": decay_channel_offset, "correction_rate_offset": correction_rate_offset, "extra_head_log_decay": extra_head_log_decay, "head_norm_gain": head_norm_gain, "mixer_output_weight": mixer_output_weight, "expert_layer_input": expert_layer_input, "feedforward_norm_gain": feedforward_norm_gain, "group_router_weight": group_router_weight, "expert_router_weight": expert_router_weight, "routes": routes, "expert_gate_weight": expert_gate_weight, "expert_up_weight": expert_up_weight, "expert_down_weight": expert_down_weight}


key_eps = 1e-06
group_eps = 0.00064
norm_eps = 1e-06
highest = lax.Precision.HIGHEST

def token_mixer_block(receptance, key_matrix, value_matrix, decay_data_term, correction_rate_data, output_gate_input, decay_channel_offset, correction_rate_offset, extra_head_log_decay, head_norm_gain, mixer_output_weight):
    positions = receptance.shape[0]

    def head_view(tensor_in):
        return tensor_in.astype(jnp.float32).reshape(positions, HEADS, HEAD_DIM)
    recept = head_view(receptance)
    keyed = head_view(key_matrix)
    valued = head_view(value_matrix)
    unit_keys = keyed * lax.rsqrt(lax.optimization_barrier(jnp.sum(keyed * keyed, axis=-1, keepdims=True)) + key_eps)
    learn_rate = jax.nn.sigmoid(head_view(correction_rate_data) + correction_rate_offset.reshape(HEADS, HEAD_DIM))
    decay_preactivation = head_view(decay_data_term) + decay_channel_offset.reshape(HEADS, HEAD_DIM)
    decay_factor = jnp.exp(-jnp.exp(-jax.nn.softplus(-decay_preactivation) - 0.5) + extra_head_log_decay[:, :, None])
    removal = unit_keys * learn_rate

    def advance(state, inputs):
        recept_now, decay_now, unit_now, removal_now, key_now, value_now = inputs
        along = jnp.einsum('hvk,hk->hv', state, unit_now, precision=highest)
        state = state * decay_now[:, None, :] - along[:, :, None] * removal_now[:, None, :] + value_now[:, :, None] * key_now[:, None, :]
        return (state, jnp.einsum('hvk,hk->hv', state, recept_now, precision=highest))
    start_state = jnp.zeros((HEADS, HEAD_DIM, HEAD_DIM), jnp.float32)
    _, head_out = lax.scan(advance, start_state, (recept, decay_factor, unit_keys, removal, keyed, valued))
    centre = lax.optimization_barrier(jnp.mean(head_out, axis=-1, keepdims=True))
    spread = lax.optimization_barrier(jnp.mean(jnp.square(head_out - centre), axis=-1, keepdims=True))
    normed = (head_out - centre) * lax.rsqrt(spread + group_eps)
    gated = normed * head_norm_gain.reshape(HEADS, HEAD_DIM) * jax.nn.sigmoid(head_view(output_gate_input))
    mixed_hidden = gated.reshape(positions, MIX).astype(jnp.bfloat16)
    hidden_groups = jnp.moveaxis(mixed_hidden.reshape(positions, N_TP, MIX // N_TP), 1, 0)
    weight_groups = mixer_output_weight.reshape(N_TP, MIX // N_TP, D)

    def add_group(total, pair):
        block_hidden, block_weight = pair
        part = jnp.dot(block_hidden, block_weight, preferred_element_type=jnp.float32).astype(jnp.bfloat16)
        part = lax.optimization_barrier(part)
        return (total + part.astype(jnp.float32), None)
    total, _ = lax.scan(add_group, jnp.zeros((positions, D), jnp.float32), (hidden_groups, weight_groups))
    return total.astype(jnp.bfloat16)

def expert_block(expert_layer_input, feedforward_norm_gain, group_router_weight, expert_router_weight, routes, expert_gate_weight, expert_up_weight, expert_down_weight):
    tokens = expert_layer_input.shape[0]
    widened = expert_layer_input.astype(jnp.float32)
    normed_input = (widened * lax.rsqrt(lax.optimization_barrier(jnp.mean(widened * widened, axis=-1, keepdims=True)) + norm_eps) * feedforward_norm_gain).astype(jnp.bfloat16)
    group_logit = jnp.dot(normed_input, group_router_weight, preferred_element_type=jnp.float32)
    group_exp = jnp.exp(group_logit)
    group_prob = group_exp / lax.optimization_barrier(jnp.sum(group_exp, axis=-1, keepdims=True))
    expert_logit = jnp.dot(normed_input, expert_router_weight, preferred_element_type=jnp.float32)
    per_group = EXPERTS // GROUPS
    chosen_logit = jnp.take_along_axis(expert_logit, routes, axis=1)
    chosen_group = jnp.take_along_axis(group_prob, routes // per_group, axis=1)
    route_weight = chosen_group * jax.nn.sigmoid(chosen_logit - chosen_logit[:, ::-1])
    flat_routes = routes.reshape(-1)
    onehot = (flat_routes[:, None] == jnp.arange(EXPERTS, dtype=jnp.int32)[None, :]).astype(jnp.int32)
    ranked = lax.optimization_barrier(jnp.sum((jnp.cumsum(onehot, axis=0) - onehot) * onehot, axis=1))
    room = N_EP * CAP
    destination = (flat_routes * room + ranked).astype(jnp.int32)
    source_rows = jnp.zeros((EXPERTS * room,), jnp.int32).at[destination].set((jnp.arange(flat_routes.shape[0], dtype=jnp.int32) // TOP).astype(jnp.int32))
    gathered = normed_input[source_rows].reshape(EXPERTS, room, D)

    def run_expert(pack):
        rows_in, gate_mat, up_mat, down_mat = pack
        gate_val = jnp.dot(rows_in, gate_mat, preferred_element_type=jnp.float32)
        up_val = jnp.dot(rows_in, up_mat, preferred_element_type=jnp.float32)
        expert_hidden = (jax.nn.silu(gate_val) * up_val).astype(jnp.bfloat16)
        hidden_groups = expert_hidden.reshape(room, N_TP, FF // N_TP)
        down_groups = down_mat.reshape(N_TP, FF // N_TP, D)
        total = jnp.zeros((room, D), jnp.float32)
        for member in range(N_TP):
            part = jnp.dot(hidden_groups[:, member], down_groups[member], preferred_element_type=jnp.float32).astype(jnp.bfloat16)
            part = lax.optimization_barrier(part)
            total = total + part.astype(jnp.float32)
        return total.astype(jnp.bfloat16)
    expert_rows = lax.map(run_expert, (gathered, expert_gate_weight, expert_up_weight, expert_down_weight)).reshape(EXPERTS * room, D)
    picked = expert_rows[destination].astype(jnp.float32).reshape(tokens, TOP, D)
    return lax.optimization_barrier(jnp.sum(picked * route_weight[:, :, None], axis=1)).astype(jnp.bfloat16)

def reference(receptance, key_matrix, value_matrix, decay_data_term, correction_rate_data, output_gate_input, decay_channel_offset, correction_rate_offset, extra_head_log_decay, head_norm_gain, mixer_output_weight, expert_layer_input, feedforward_norm_gain, group_router_weight, expert_router_weight, routes, expert_gate_weight, expert_up_weight, expert_down_weight):
    token_mixer_output = token_mixer_block(receptance, key_matrix, value_matrix, decay_data_term, correction_rate_data, output_gate_input, decay_channel_offset, correction_rate_offset, extra_head_log_decay, head_norm_gain, mixer_output_weight)
    expert_out = expert_block(expert_layer_input, feedforward_norm_gain, group_router_weight, expert_router_weight, routes, expert_gate_weight, expert_up_weight, expert_down_weight)
    return (token_mixer_output, expert_out)
```

```python
import functools
import jax
import jax.numpy as jnp
from jax import lax
from jax.experimental import pallas as pl
from jax.experimental.pallas import tpu as pltpu
from jax.sharding import PartitionSpec as P

HEAD_DIM = 64
GROUPS = 4
PARTS = 1
key_eps = 1e-06
group_eps = 0.00064
norm_eps = 1e-06
BASE = 16

f32, bf16 = jnp.float32, jnp.bfloat16
NN = (((1,), (0,)), ((), ()))
NT = (((1,), (1,)), ((), ()))
TN = (((0,), (0,)), ((), ()))


def mm(a, b, dims=NN):
    return lax.dot_general(a, b, dims, preferred_element_type=f32)


def halves(x):
    high = x.astype(bf16)
    return high, (x - high.astype(f32)).astype(bf16)


def thirds(x):
    high = x.astype(bf16)
    rest = x - high.astype(f32)
    mid = rest.astype(bf16)
    return high, mid, (rest - mid.astype(f32)).astype(bf16)


def exact_right(x, ones, parts):
    return sum(mm(p, ones) for p in parts(x))


def exact_left(ones, x, parts):
    return sum(mm(ones, p) for p in parts(x))


def iota(shape, axis):
    return lax.broadcasted_iota(jnp.int32, shape, axis)


def head_mask(lanes):
    return iota((lanes, lanes), 0) // HEAD_DIM == iota((lanes, lanes), 1) // HEAD_DIM


def spread(x, mask):
    rep = mask.shape[0] // HEAD_DIM
    return jnp.where(mask, jnp.concatenate([x] * rep, axis=0), jnp.zeros((), x.dtype))


def fold(x):
    pieces = [x[i : i + HEAD_DIM] for i in range(0, x.shape[0], HEAD_DIM)]
    return functools.reduce(jnp.add, pieces)


def mixer_kernel(
    q_ref, k_ref, v_ref, w_ref, a_ref, wo_ref, ao_ref, ex_ref,
    local_ref, reach_ref, end_ref,
    u_s, r_s, c_s, ld_s, pair_s, diag_s, tri_s, ue_s, qe_s, kh_s, rh_s, up_s, qp_s, g_s, et_s,
):
    rows, lanes = q_ref.shape
    C = HEAD_DIM
    chunks = rows // C
    heads = lanes // HEAD_DIM
    hm = head_mask(lanes)
    ones_bd = hm.astype(bf16)

    k = k_ref[...].astype(f32)
    u = k * lax.rsqrt(exact_right(k * k, ones_bd, halves) + key_eps)
    u_s[...] = u
    r_s[...] = u * jax.nn.sigmoid(a_ref[...].astype(f32) + ao_ref[...])
    owner = (iota((heads, lanes), 1) // HEAD_DIM == iota((heads, lanes), 0)).astype(bf16)
    exb = sum(mm(p, owner, TN) for p in thirds(ex_ref[...]))
    pre = w_ref[...].astype(f32) + wo_ref[...]
    ld_s[...] = exb - jax.nn.sigmoid(pre) * 0.6065306597126334

    tri = (iota((C, C), 0) >= iota((C, C), 1)).astype(bf16)
    same = head_mask(lanes)
    rr, cc = iota((lanes, lanes), 0), iota((lanes, lanes), 1)
    strict = jnp.logical_and(same, rr > cc)
    upto = jnp.logical_and(same, rr >= cc)
    base_mask = rr // BASE == cc // BASE

    def first(i, _):
        at = pl.ds(pl.multiple_of(i * C, C), C)
        ld = ld_s[at, :]
        c = exact_left(tri, ld, thirds)
        tot = c[C - 1 : C, :]
        mid = 0.5 * tot
        em = jnp.exp(mid)
        eq = jnp.exp(c - mid)
        eu = jnp.exp(c - ld - mid)
        ek = jnp.exp(mid - c)
        ut, qt = u_s[at, :] * eu, q_ref[at, :].astype(f32) * eq
        kt, rt = k_ref[at, :].astype(f32) * ek, r_s[at, :] * ek
        ue_s[at, :] = (ut * em).astype(bf16)
        qe_s[at, :] = qt * em
        kh_s[at, :] = (kt * em).astype(bf16)
        rh_s[at, :] = (rt * em).astype(bf16)
        et_s[pl.ds(i, 1), :] = em * em
        left = jnp.concatenate([spread(ut.astype(bf16), hm), spread(qt.astype(bf16), hm)], axis=0)
        right = jnp.concatenate([spread(kt.astype(bf16), hm), spread(rt.astype(bf16), hm)], axis=0)
        pairs = mm(left, right, NT)
        uk = jnp.where(strict, pairs[:lanes, :lanes], 0.0)
        ur = jnp.where(strict, pairs[:lanes, lanes:], 0.0)
        qk = jnp.where(upto, pairs[lanes:, :lanes], 0.0)
        qr = jnp.where(upto, pairs[lanes:, lanes:], 0.0)
        pair_s[i, 0] = uk.astype(bf16)
        pair_s[i, 1] = ur.astype(bf16)
        pair_s[i, 2] = qk.astype(bf16)
        pair_s[i, 3] = qr.astype(bf16)
        dg = jnp.where(base_mask, ur, 0.0)
        diag_s[i] = functools.reduce(
            jnp.add, [dg[p : p + BASE] for p in range(0, lanes, BASE)]
        )
        return 0

    lax.fori_loop(0, chunks, first, 0, unroll=2)

    dparts = thirds(diag_s[...].reshape(chunks * BASE, lanes))
    t = jnp.where(
        iota((chunks, BASE, lanes), 1) == iota((chunks, BASE, lanes), 2) % BASE, 1.0, 0.0
    ).astype(f32)
    for j in range(BASE - 1):
        pick = jnp.logical_and(base_mask, rr % BASE == j).astype(bf16)
        col = sum(mm(p, pick) for p in dparts).reshape(chunks, BASE, lanes)
        t = t - col * t[:, j : j + 1, :]
    tri_s[...] = t

    m32 = jnp.logical_and(rr // (2 * BASE) == cc // (2 * BASE), jnp.logical_not(base_mask))
    m64 = rr // (2 * BASE) != cc // (2 * BASE)
    pickv = (iota((HEAD_DIM, lanes), 0) == iota((HEAD_DIM, lanes), 1) % HEAD_DIM).astype(bf16)
    zero = jnp.zeros((), bf16)

    def second(i, _):
        at = pl.ds(pl.multiple_of(i * C, C), C)
        uk, ur, qk, qr = pair_s[i, 0], pair_s[i, 1], pair_s[i, 2], pair_s[i, 3]
        td = tri_s[i]
        t16 = jnp.where(base_mask, jnp.concatenate([td] * (lanes // BASE), axis=0), 0.0)
        t16b = t16.astype(bf16)
        p1 = mm(jnp.where(m32, ur, zero), t16b).astype(bf16)
        t32 = t16 - mm(t16b, p1)
        t32b = t32.astype(bf16)
        p2 = mm(jnp.where(m64, ur, zero), t32b).astype(bf16)
        t64 = (t32 - mm(t32b, p2)).astype(bf16)
        ubd = spread(ue_s[at, :], hm)
        ta = mm(t64, uk).astype(bf16)
        up = mm(t64, ubd).astype(bf16)
        up_s[i] = up
        vbd = spread(v_ref[at, :], hm)
        za = mm(ta, vbd)
        o = mm(qk, vbd) - mm(qr, za.astype(bf16))
        local_ref[at, :] = fold(o)
        qp_s[at, :] = (qe_s[at, :] - fold(mm(qr, up))).astype(bf16)
        vt = mm(pickv, vbd, NT).astype(bf16)
        zat = mm(vt, ta, NT).astype(bf16)
        g_s[i] = mm(vt, spread(kh_s[at, :], hm)) - mm(zat, spread(rh_s[at, :], hm))
        return 0

    lax.fori_loop(0, chunks, second, 0, unroll=2)

    def third(i, x):
        at = pl.ds(pl.multiple_of(i * C, C), C)
        xb = x.astype(bf16)
        xs, xm = xb[:HEAD_DIM], xb[HEAD_DIM:]
        qp = qp_s[at, :]
        local_ref[at, :] += mm(qp, spread(xs, hm), NT)
        reach_ref[at, :] = mm(qp, spread(xm, hm), NT).astype(bf16)
        at_ = mm(xb, up_s[i], NT).astype(bf16)
        corr = mm(at_, spread(rh_s[at, :], hm))
        g = g_s[i]
        return x * et_s[pl.ds(i, 1), :] + jnp.concatenate([g, jnp.zeros_like(g)], axis=0) - corr

    x0 = jnp.concatenate([jnp.zeros((HEAD_DIM, lanes), f32), pickv.astype(f32)], axis=0)
    x = lax.fori_loop(0, chunks, third, x0, unroll=2)
    end_ref[...] = x.astype(bf16)


def mixer_local(q, k, v, w, a, wo, ao, ex):
    rows, lanes = q.shape
    chunks = rows // HEAD_DIM
    V = pltpu.VMEM
    return pl.pallas_call(
        mixer_kernel,
        out_shape=(
            jax.ShapeDtypeStruct((rows, lanes), f32),
            jax.ShapeDtypeStruct((rows, lanes), bf16),
            jax.ShapeDtypeStruct((2 * HEAD_DIM, lanes), bf16),
        ),
        scratch_shapes=[
            V((rows, lanes), f32), V((rows, lanes), f32), V((8, 128), f32), V((rows, lanes), f32),
            V((chunks, 4, lanes, lanes), bf16), V((chunks, BASE, lanes), f32), V((chunks, BASE, lanes), f32),
            V((rows, lanes), bf16), V((rows, lanes), f32), V((rows, lanes), bf16), V((rows, lanes), bf16),
            V((chunks, lanes, lanes), bf16), V((rows, lanes), bf16), V((chunks, HEAD_DIM, lanes), f32),
            V((chunks, lanes), f32),
        ],
        compiler_params=pltpu.CompilerParams(vmem_limit_bytes=40 * 1024 * 1024),
        cost_estimate=pl.CostEstimate(flops=30_000_000_000, bytes_accessed=4_000_000, transcendentals=0),
        name="mixer_local",
    )(q, k, v, w, a, wo.reshape(1, -1), ao.reshape(1, -1), ex)


def finish_kernel(place_ref, ends_ref, local_ref, reach_ref, gate_ref, gain_ref, out_ref, mixed_s):
    devices, _, lanes = ends_ref.shape
    hm = head_mask(lanes)
    ones_bd = hm.astype(bf16)
    place = place_ref[0]

    def hop(e, s):
        pbd = spread(ends_ref[e, HEAD_DIM:, :], hm)
        new = sum(mm(p, pbd) for p in halves(s)) + ends_ref[e, :HEAD_DIM, :].astype(f32)
        return jnp.where(e < place, new, s)

    s = lax.fori_loop(0, devices - 1, hop, jnp.zeros((HEAD_DIM, lanes), f32), unroll=True)
    head_out = local_ref[...] + mm(reach_ref[...], spread(s.astype(bf16), hm), NT)
    centred = head_out - exact_right(head_out, ones_bd, halves) * (1.0 / HEAD_DIM)
    var = exact_right(centred * centred, ones_bd, halves) * (1.0 / HEAD_DIM)
    gate = jax.nn.sigmoid(gate_ref[...].astype(f32))
    mixed_s[...] = centred * lax.rsqrt(var + group_eps) * gain_ref[...] * gate
    count, rows, _ = out_ref.shape
    for m in range(count):
        at = pl.multiple_of(lax.bitwise_xor(place_ref[1], m) * rows, rows)
        out_ref[m] = mixed_s[pl.ds(at, rows), :].astype(bf16)


def mixer_finish(place, ends, local, reach, gate, gain, count):
    vm = pl.BlockSpec(memory_space=pltpu.VMEM)
    return pl.pallas_call(
        finish_kernel,
        out_shape=jax.ShapeDtypeStruct((count, local.shape[0] // count, local.shape[1]), bf16),
        in_specs=[pl.BlockSpec(memory_space=pltpu.SMEM)] + [vm] * 5,
        out_specs=vm,
        scratch_shapes=[pltpu.VMEM(local.shape, f32)],
        compiler_params=pltpu.CompilerParams(vmem_limit_bytes=24 * 1024 * 1024),
        cost_estimate=pl.CostEstimate(flops=4_000_000_000, bytes_accessed=2_000_000, transcendentals=0),
        name="mixer_finish",
    )(place, ends, local, reach, gate, gain.reshape(1, -1))


def route_kernel(place_ref, x_ref, gain_ref, gw_ref, ew_ref, routes_ref, *outs):
    send_refs, info_ref = outs[:-1], outs[-1]
    tokens, width = x_ref.shape
    experts, part, share = send_refs[0].shape
    per_group = experts // GROUPS
    x = x_ref[...].astype(f32)
    scale = lax.rsqrt(jnp.mean(x * x, axis=-1, keepdims=True) + norm_eps)
    normed = (x * scale * gain_ref[...]).astype(bf16)
    group_exp = jnp.exp(mm(gw_ref[...], normed, NT))
    group_prob = group_exp / jnp.sum(group_exp, axis=0, keepdims=True)
    logit = mm(ew_ref[...], normed, NT)
    top = routes_ref.shape[0]
    ids = [routes_ref[k : k + 1, :] for k in range(top)]
    match = [iota((experts, tokens), 0) == i for i in ids]
    chosen = [jnp.sum(jnp.where(m, logit, 0.0), axis=0, keepdims=True) for m in match]
    group = [
        jnp.sum(
            jnp.where(iota((GROUPS, tokens), 0) == i // per_group, group_prob, 0.0),
            axis=0, keepdims=True,
        )
        for i in ids
    ]
    weights = [group[k] * jax.nn.sigmoid(chosen[k] - chosen[top - 1 - k]) for k in range(top)]
    counts = sum(m.astype(f32) for m in match)
    earlier = (iota((tokens, tokens), 0) < iota((tokens, tokens), 1)).astype(bf16)
    before = mm(counts.astype(bf16), earlier)
    placed = [jnp.sum(jnp.where(m, before, 0.0), axis=0, keepdims=True) for m in match]
    rows = weights + placed + [i.astype(f32) for i in ids]
    rows += [jnp.zeros((1, tokens), f32)] * (8 - len(rows))
    info_ref[...] = jnp.transpose(jnp.concatenate(rows, axis=0))
    own = pl.multiple_of(place_ref[0] * share, share)
    mine = (
        x_ref[:, pl.ds(own, share)].astype(f32) * scale * gain_ref[:, pl.ds(own, share)]
    ).astype(bf16)
    slots = iota((experts * part, tokens), 0)
    for j, send_ref in enumerate(send_refs):
        hit = None
        for i, p in zip(ids, placed):
            p = p.astype(jnp.int32)
            inside = jnp.logical_and(p >= j * part, p < (j + 1) * part)
            h = jnp.logical_and(slots == i * part + p - j * part, inside)
            hit = h if hit is None else jnp.logical_or(hit, h)
        send_ref[...] = mm(hit.astype(bf16), mine).astype(bf16).reshape(experts, part, share)


def route(place, x, gain, gw, ew, routes, parts, part, share):
    experts, tokens = ew.shape[0], x.shape[0]
    vm = pl.BlockSpec(memory_space=pltpu.VMEM)
    return pl.pallas_call(
        route_kernel,
        out_shape=[jax.ShapeDtypeStruct((experts, part, share), bf16)] * parts
        + [jax.ShapeDtypeStruct((tokens, 8), f32)],
        in_specs=[pl.BlockSpec(memory_space=pltpu.SMEM)] + [vm] * 5,
        out_specs=[vm] * (parts + 1),
        compiler_params=pltpu.CompilerParams(vmem_limit_bytes=24 * 1024 * 1024),
        cost_estimate=pl.CostEstimate(flops=4_000_000_000, bytes_accessed=1_000_000, transcendentals=0),
        name="route",
    )(place, x, gain.reshape(1, -1), gw, ew, routes)


def combine_kernel(info_ref, *refs, top):
    homes, out_ref = refs[:-1], refs[-1]
    tokens = info_ref.shape[0]
    experts, part, share = homes[0].shape
    slots = iota((tokens, experts * part), 1)
    total = jnp.zeros((tokens, share), f32)
    for k in range(top):
        p = info_ref[:, top + k : top + k + 1].astype(jnp.int32)
        i = info_ref[:, 2 * top + k : 2 * top + k + 1].astype(jnp.int32)
        rows = jnp.zeros((tokens, share), f32)
        for j, home in enumerate(homes):
            inside = jnp.logical_and(p >= j * part, p < (j + 1) * part)
            h = jnp.logical_and(slots == i * part + p - j * part, inside)
            rows += mm(h.astype(bf16), home[...].reshape(experts * part, share))
        total += info_ref[:, k : k + 1] * rows
    out_ref[...] = total.astype(bf16)


def combine(info, homes, top):
    vm = pl.BlockSpec(memory_space=pltpu.VMEM)
    return pl.pallas_call(
        functools.partial(combine_kernel, top=top),
        out_shape=jax.ShapeDtypeStruct((info.shape[0], homes[0].shape[2]), bf16),
        in_specs=[vm] * (1 + len(homes)),
        out_specs=vm,
        compiler_params=pltpu.CompilerParams(vmem_limit_bytes=24 * 1024 * 1024),
        cost_estimate=pl.CostEstimate(flops=1_000_000_000, bytes_accessed=1_000_000, transcendentals=0),
        name="combine",
    )(info, *homes)


def tile_of(size, most):
    return most if size % most == 0 else size


def hidden_kernel(place_ref, *refs, masks):
    xs, (wg_ref, wu_ref, out_ref) = refs[: len(masks)], refs[len(masks) :]
    share = xs[0].shape[1]
    gate = up = None
    for m, x in zip(masks, xs):
        at = pl.ds(pl.multiple_of(lax.bitwise_xor(place_ref[0], m) * share, share), share)
        g, u = mm(x[...], wg_ref[0, at, :]), mm(x[...], wu_ref[0, at, :])
        gate, up = (g, u) if gate is None else (gate + g, up + u)
    out_ref[...] = (gate * jax.nn.sigmoid(gate) * up).astype(bf16)


def hidden(place, masks, xs, wg, wu):
    rows, share = xs[0].shape
    _, width, units = wg.shape
    tile = tile_of(units, 256)
    weight = pl.BlockSpec((1, width, tile), lambda f, p: (0, 0, f))
    return pl.pallas_call(
        functools.partial(hidden_kernel, masks=masks),
        grid_spec=pltpu.PrefetchScalarGridSpec(
            num_scalar_prefetch=1,
            grid=(units // tile,),
            in_specs=[pl.BlockSpec((rows, share), lambda f, p: (0, 0))] * len(xs) + [weight] * 2,
            out_specs=pl.BlockSpec((rows, tile), lambda f, p: (0, f)),
        ),
        out_shape=jax.ShapeDtypeStruct((rows, units), bf16),
        compiler_params=pltpu.CompilerParams(vmem_limit_bytes=32 * 1024 * 1024),
        cost_estimate=pl.CostEstimate(
            flops=4 * rows * width * units, bytes_accessed=4 * width * units, transcendentals=0
        ),
        name="hidden",
    )(place, *xs, wg, wu)


def down_kernel(place_ref, h_ref, w_ref, out_ref):
    out_ref[0] = mm(h_ref[...], w_ref[0]).astype(bf16)


def down(place, masks, h, wd, share):
    rows, units = h.shape
    masks = tuple(masks)

    def column(i, p):
        mask = jnp.int32(masks[-1])
        for j in range(len(masks) - 2, -1, -1):
            mask = jnp.where(i == j, jnp.int32(masks[j]), mask)
        return 0, 0, lax.bitwise_xor(p[0], mask)

    return pl.pallas_call(
        down_kernel,
        grid_spec=pltpu.PrefetchScalarGridSpec(
            num_scalar_prefetch=1,
            grid=(len(masks),),
            in_specs=[
                pl.BlockSpec((rows, units), lambda i, p: (0, 0)),
                pl.BlockSpec((1, units, share), column),
            ],
            out_specs=pl.BlockSpec((1, rows, share), lambda i, p: (i, 0, 0)),
        ),
        out_shape=jax.ShapeDtypeStruct((len(masks), rows, share), bf16),
        compiler_params=pltpu.CompilerParams(vmem_limit_bytes=24 * 1024 * 1024),
        cost_estimate=pl.CostEstimate(
            flops=2 * rows * units * share * len(masks),
            bytes_accessed=2 * units * share * len(masks), transcendentals=0,
        ),
        name="down",
    )(place, h, wd)


def project_kernel(*refs):
    out_ref = refs[-1]
    count = (len(refs) - 1) // 2
    total = None
    for x, w in zip(refs[:count], refs[count:-1]):
        p = mm(x[...], w[...]).astype(bf16).astype(f32)
        total = p if total is None else total + p
    out_ref[...] = total.astype(bf16)


def project(xs, ws):
    rows, lanes = xs[0].shape
    width = ws[0].shape[1]
    tile = tile_of(width, 512)
    return pl.pallas_call(
        project_kernel,
        grid=(width // tile,),
        in_specs=[pl.BlockSpec((rows, lanes), lambda i: (0, 0))] * len(xs)
        + [pl.BlockSpec((lanes, tile), lambda i: (0, i))] * len(ws),
        out_specs=pl.BlockSpec((rows, tile), lambda i: (0, i)),
        out_shape=jax.ShapeDtypeStruct((rows, width), bf16),
        compiler_params=pltpu.CompilerParams(vmem_limit_bytes=24 * 1024 * 1024),
        cost_estimate=pl.CostEstimate(
            flops=2 * rows * lanes * width * len(xs),
            bytes_accessed=2 * lanes * width * len(xs), transcendentals=0,
        ),
        name="project",
    )(*xs, *ws)


def swap(x, mask):
    count = lax.axis_size("tp")
    return lax.ppermute(x, "tp", [(i, i ^ mask) for i in range(count)])


def gathered(x, far=None):
    masks, blocks = [0], [x]
    mask = lax.axis_size("tp") // 2
    if far is not None:
        masks, blocks, mask = [0, mask], [x, far], mask // 2
    while mask:
        blocks += [swap(b, mask) for b in blocks]
        masks += [m ^ mask for m in masks]
        mask //= 2
    return tuple(masks), blocks


def local(
    receptance, key_matrix, value_matrix, decay_data_term, correction_rate_data,
    output_gate_input, decay_channel_offset, correction_rate_offset, extra_head_log_decay,
    head_norm_gain, mixer_output_weight, expert_layer_input, feedforward_norm_gain,
    group_router_weight, expert_router_weight, routes, expert_gate_weight, expert_up_weight,
    expert_down_weight,
):
    ep, tp = lax.axis_size("ep"), lax.axis_size("tp")
    place = lax.axis_index("tp").reshape(1).astype(jnp.int32)
    turn = lax.axis_index("ep").reshape(1).astype(jnp.int32)
    tokens, width = expert_layer_input.shape
    experts = expert_router_weight.shape[1]
    share = width // tp
    capacity = 4 * tokens // ep
    part = capacity // PARTS

    *sends, info = route(
        place, expert_layer_input, feedforward_norm_gain, group_router_weight.T,
        expert_router_weight.T, routes.T, PARTS, part, share,
    )
    arrived = [lax.all_to_all(s, "ep", split_axis=0, concat_axis=0, tiled=True) for s in sends]
    masks, blocks = [0], [mixer_output_weight]
    top_mask = tp // 2
    far = swap(mixer_output_weight, top_mask)

    local_read, reached, end = mixer_local(
        receptance, key_matrix, value_matrix, decay_data_term, correction_rate_data,
        decay_channel_offset, correction_rate_offset, extra_head_log_decay.T,
    )
    arrived, far, end = lax.optimization_barrier((arrived, far, end))
    weight_masks, weight_blocks = gathered(mixer_output_weight, far)
    ends = lax.all_to_all(
        jnp.broadcast_to(end[None], (ep,) + end.shape), "ep", split_axis=0, concat_axis=0, tiled=True
    )

    waiting = []
    for piece in arrived:
        masks, blocks = gathered(piece.reshape(experts * part, share))
        h = hidden(place, masks, blocks, expert_gate_weight, expert_up_weight)
        todo, bit = list(range(tp)), 1
        odd = [m for m in todo if m & bit]
        even = [m for m in todo if not m & bit]
        send = down(place, odd, h, expert_down_weight, share)
        keep = down(place, even, h, expert_down_weight, share)
        while True:
            got = swap(send, bit)
            bit *= 2
            if bit >= tp:
                break
            total = (keep.astype(f32) + got.astype(f32)).astype(bf16)
            total = total.reshape((-1, 2) + total.shape[1:])
            keep, send = total[:, 0], total[:, 1]
        waiting.append((keep, got))

    mixed = mixer_finish(
        jnp.concatenate([turn, place]), ends, local_read, reached, output_gate_input, head_norm_gain, tp
    )
    pieces = [mixed[m] if m == 0 else swap(mixed[m], m) for m in weight_masks]
    token_mixer_output = project(pieces, weight_blocks)
    waiting, token_mixer_output = lax.optimization_barrier((waiting, token_mixer_output))
    homes = []
    for keep, got in waiting:
        total = (keep.astype(f32) + got.astype(f32)).astype(bf16).reshape(experts, part, share)
        homes.append(lax.all_to_all(total, "ep", split_axis=0, concat_axis=0, tiled=True))
    expert_out = combine(info, homes, routes.shape[1])
    return (token_mixer_output, expert_out)


def solution(mesh):
    in_specs = (
        P("ep", "tp"), P("ep", "tp"), P("ep", "tp"), P("ep", "tp"), P("ep", "tp"), P("ep", "tp"),
        P("tp"), P("tp"), P("ep", "tp"), P("tp"), P("tp", None), P("ep", None), P(), P(), P(),
        P("ep", None), P("ep", None, "tp"), P("ep", None, "tp"), P("ep", "tp", None),
    )
    out_specs = (P(("ep", "tp"), None), P("ep", "tp"))
    return jax.shard_map(local, mesh=mesh, in_specs=in_specs, out_specs=out_specs, check_vma=False)
```

```python
import functools
import jax
import jax.numpy as jnp
from jax import lax
from jax.experimental import pallas as pl
from jax.experimental.pallas import tpu as pltpu
from jax.sharding import PartitionSpec as P

HEAD_DIM = 64
GROUPS = 4
VMEM_LIMIT = 16 * 1024 * 1024
key_eps = 1e-06
group_eps = 0.00064
norm_eps = 1e-06
BASE = 16

f32, bf16 = jnp.float32, jnp.bfloat16
NN = (((1,), (0,)), ((), ()))
NT = (((1,), (1,)), ((), ()))
TN = (((0,), (0,)), ((), ()))


def hbm(*arrays):
    return [pltpu.with_memory_space_constraint(a, pltpu.HBM) for a in arrays]


def mm(a, b, dims=NN):
    return lax.dot_general(a, b, dims, preferred_element_type=f32)


def halves(x):
    high = x.astype(bf16)
    return high, (x - high.astype(f32)).astype(bf16)


def thirds(x):
    high = x.astype(bf16)
    rest = x - high.astype(f32)
    mid = rest.astype(bf16)
    return high, mid, (rest - mid.astype(f32)).astype(bf16)


def exact_right(x, ones, parts):
    return sum(mm(p, ones) for p in parts(x))


def exact_left(ones, x, parts):
    return sum(mm(ones, p) for p in parts(x))


def iota(shape, axis):
    return lax.broadcasted_iota(jnp.int32, shape, axis)


def head_mask(lanes):
    return iota((lanes, lanes), 0) // HEAD_DIM == iota((lanes, lanes), 1) // HEAD_DIM


def spread(x, mask):
    rep = mask.shape[0] // HEAD_DIM
    return jnp.where(mask, jnp.concatenate([x] * rep, axis=0), jnp.zeros((), x.dtype))


def fold(x):
    pieces = [x[i : i + HEAD_DIM] for i in range(0, x.shape[0], HEAD_DIM)]
    return functools.reduce(jnp.add, pieces)


def mixer_kernel(
    first_part, last_part, q_ref, k_ref, v_ref, w_ref, a_ref, wo_ref, ao_ref, ex_ref, *refs
):
    refs = list(refs)
    start_ref = None if first_part else refs.pop(0)
    local_ref, reach_ref, end_ref = refs[:3]
    (
        u_s, r_s, ld_s, pair_s, diag_s, tri_s, ue_s, qe_s, kh_s, rh_s, up_s, qp_s, g_s, et_s,
    ) = refs[3:]
    rows, lanes = q_ref.shape
    C = HEAD_DIM
    chunks = rows // C
    heads = lanes // HEAD_DIM
    hm = head_mask(lanes)
    ones_bd = hm.astype(bf16)

    k = k_ref[...].astype(f32)
    u = k * lax.rsqrt(exact_right(k * k, ones_bd, halves) + key_eps)
    u_s[...] = u
    r_s[...] = u * jax.nn.sigmoid(a_ref[...].astype(f32) + ao_ref[...])
    owner = (iota((heads, lanes), 1) // HEAD_DIM == iota((heads, lanes), 0)).astype(bf16)
    exb = sum(mm(p, owner, TN) for p in thirds(ex_ref[...]))
    pre = w_ref[...].astype(f32) + wo_ref[...]
    ld_s[...] = exb - jax.nn.sigmoid(pre) * 0.6065306597126334

    tri = (iota((C, C), 0) >= iota((C, C), 1)).astype(bf16)
    same = head_mask(lanes)
    rr, cc = iota((lanes, lanes), 0), iota((lanes, lanes), 1)
    strict = jnp.logical_and(same, rr > cc)
    upto = jnp.logical_and(same, rr >= cc)
    base_mask = rr // BASE == cc // BASE

    def first(i, _):
        at = pl.ds(pl.multiple_of(i * C, C), C)
        ld = ld_s[at, :]
        c = exact_left(tri, ld, thirds)
        tot = c[C - 1 : C, :]
        mid = 0.5 * tot
        em = jnp.exp(mid)
        eq = jnp.exp(c - mid)
        eu = jnp.exp(c - ld - mid)
        ek = jnp.exp(mid - c)
        ut, qt = u_s[at, :] * eu, q_ref[at, :].astype(f32) * eq
        kt, rt = k_ref[at, :].astype(f32) * ek, r_s[at, :] * ek
        ue_s[at, :] = (ut * em).astype(bf16)
        qe_s[at, :] = qt * em
        kh_s[at, :] = (kt * em).astype(bf16)
        rh_s[at, :] = (rt * em).astype(bf16)
        et_s[pl.ds(i, 1), :] = em * em
        left = jnp.concatenate([spread(ut.astype(bf16), hm), spread(qt.astype(bf16), hm)], axis=0)
        right = jnp.concatenate([spread(kt.astype(bf16), hm), spread(rt.astype(bf16), hm)], axis=0)
        pairs = mm(left, right, NT)
        uk = jnp.where(strict, pairs[:lanes, :lanes], 0.0)
        ur = jnp.where(strict, pairs[:lanes, lanes:], 0.0)
        qk = jnp.where(upto, pairs[lanes:, :lanes], 0.0)
        qr = jnp.where(upto, pairs[lanes:, lanes:], 0.0)
        pair_s[i, 0] = uk.astype(bf16)
        pair_s[i, 1] = ur.astype(bf16)
        pair_s[i, 2] = qk.astype(bf16)
        pair_s[i, 3] = qr.astype(bf16)
        dg = jnp.where(base_mask, ur, 0.0)
        diag_s[i] = functools.reduce(
            jnp.add, [dg[p : p + BASE] for p in range(0, lanes, BASE)]
        )
        return 0

    lax.fori_loop(0, chunks, first, 0, unroll=4)

    dall = diag_s[...].reshape(chunks * BASE, lanes)
    dparts = thirds(dall)
    t = jnp.where(
        iota((chunks, BASE, lanes), 1) == iota((chunks, BASE, lanes), 2) % BASE, 1.0, 0.0
    ).astype(f32)
    for j in range(BASE - 1):
        if lanes % 128:
            pick = jnp.logical_and(base_mask, rr % BASE == j).astype(bf16)
            col = sum(mm(p, pick) for p in dparts)
        else:
            near = iota((chunks * BASE, 128), 1) // BASE * BASE + j
            col = jnp.concatenate(
                [
                    jnp.take_along_axis(dall[:, p : p + 128], near, axis=1, mode="promise_in_bounds")
                    for p in range(0, lanes, 128)
                ],
                axis=1,
            )
        col = col.reshape(chunks, BASE, lanes)
        t = t - col * t[:, j : j + 1, :]
    tri_s[...] = t

    m32 = jnp.logical_and(rr // (2 * BASE) == cc // (2 * BASE), jnp.logical_not(base_mask))
    m64 = rr // (2 * BASE) != cc // (2 * BASE)
    pickv = (iota((HEAD_DIM, lanes), 0) == iota((HEAD_DIM, lanes), 1) % HEAD_DIM).astype(bf16)
    zero = jnp.zeros((), bf16)

    def second(i, _):
        at = pl.ds(pl.multiple_of(i * C, C), C)
        uk, ur, qk, qr = pair_s[i, 0], pair_s[i, 1], pair_s[i, 2], pair_s[i, 3]
        td = tri_s[i]
        t16 = jnp.where(base_mask, jnp.concatenate([td] * (lanes // BASE), axis=0), 0.0)
        t16b = t16.astype(bf16)
        p1 = mm(jnp.where(m32, ur, zero), t16b).astype(bf16)
        t32 = t16 - mm(t16b, p1)
        t32b = t32.astype(bf16)
        p2 = mm(jnp.where(m64, ur, zero), t32b).astype(bf16)
        t64 = (t32 - mm(t32b, p2)).astype(bf16)
        ubd = spread(ue_s[at, :], hm)
        ta = mm(t64, uk).astype(bf16)
        up = mm(t64, ubd).astype(bf16)
        up_s[i] = up
        vbd = spread(v_ref[at, :], hm)
        za = mm(ta, vbd)
        o = mm(qk, vbd) - mm(qr, za.astype(bf16))
        local_ref[at, :] = fold(o)
        qp_s[at, :] = (qe_s[at, :] - fold(mm(qr, up))).astype(bf16)
        vt = mm(pickv, vbd, NT).astype(bf16)
        zat = mm(vt, ta, NT).astype(bf16)
        g_s[i] = mm(vt, spread(kh_s[at, :], hm)) - mm(zat, spread(rh_s[at, :], hm))
        return 0

    lax.fori_loop(0, chunks, second, 0, unroll=4)

    def third(i, x):
        at = pl.ds(pl.multiple_of(i * C, C), C)
        xb = x.astype(bf16)
        xs, xm = xb[:HEAD_DIM], xb[HEAD_DIM:]
        qp = qp_s[at, :]
        local_ref[at, :] += mm(qp, spread(xs, hm), NT)
        reach_ref[at, :] = mm(qp, spread(xm, hm), NT).astype(bf16)
        at_ = mm(xb, up_s[i], NT).astype(bf16)
        corr = mm(at_, spread(rh_s[at, :], hm))
        g = g_s[i]
        return x * et_s[pl.ds(i, 1), :] + jnp.concatenate([g, jnp.zeros_like(g)], axis=0) - corr

    if first_part:
        x0 = jnp.concatenate([jnp.zeros((HEAD_DIM, lanes), f32), pickv.astype(f32)], axis=0)
    else:
        x0 = start_ref[...]
    x = lax.fori_loop(0, chunks, third, x0, unroll=4)
    if last_part:
        end_ref[...] = jnp.broadcast_to(x.astype(bf16)[None], end_ref.shape)
    else:
        end_ref[...] = x


def mixer_local(part, parts, copies, start, q, k, v, w, a, wo, ao, ex):
    rows, lanes = q.shape
    rows //= parts
    chunks = rows // HEAD_DIM
    heads = ex.shape[0]
    V = pltpu.VMEM
    block = pl.BlockSpec((rows, lanes), lambda i: (part, 0))
    vector = pl.BlockSpec((1, lanes), lambda i: (0, 0))
    state = pl.BlockSpec((2 * HEAD_DIM, lanes), lambda i: (0, 0))
    out = pl.BlockSpec((rows, lanes), lambda i: (0, 0))
    last = part == parts - 1
    ends = (copies, 2 * HEAD_DIM, lanes)
    return pl.pallas_call(
        functools.partial(mixer_kernel, part == 0, last),
        grid=(1,),
        in_specs=[block] * 5
        + [vector] * 2
        + [pl.BlockSpec((heads, rows), lambda i: (0, part))]
        + ([] if start is None else [state]),
        out_specs=[out, out, pl.BlockSpec(ends, lambda i: (0, 0, 0)) if last else state],
        out_shape=[
            pltpu.HBM((rows, lanes), f32),
            pltpu.HBM((rows, lanes), bf16),
            pltpu.HBM(ends, bf16) if last else jax.ShapeDtypeStruct(ends[1:], f32),
        ],
        scratch_shapes=[
            V((rows, lanes), f32), V((rows, lanes), f32), V((rows, lanes), f32),
            V((chunks, 4, lanes, lanes), bf16), V((chunks, BASE, lanes), f32), V((chunks, BASE, lanes), f32),
            V((rows, lanes), bf16), V((rows, lanes), f32), V((rows, lanes), bf16), V((rows, lanes), bf16),
            V((chunks, lanes, lanes), bf16), V((rows, lanes), bf16), V((chunks, HEAD_DIM, lanes), f32),
            V((chunks, lanes), f32),
        ],
        compiler_params=pltpu.CompilerParams(vmem_limit_bytes=VMEM_LIMIT),
        cost_estimate=pl.CostEstimate(flops=10_000_000_000, bytes_accessed=2_000_000, transcendentals=0),
        name="mixer_local",
    )(
        *hbm(q, k, v, w, a, wo.reshape(1, -1), ao.reshape(1, -1), ex),
        *([] if start is None else [start]),
    )


def finish_kernel(place_ref, ends_ref, gate_ref, gain_ref, *refs):
    out_ref, mixed_s = refs[-2:]
    parts = (len(refs) - 2) // 2
    devices, _, lanes = ends_ref.shape
    hm = head_mask(lanes)
    ones_bd = hm.astype(bf16)
    place = place_ref[1]

    def hop(e, s):
        pbd = spread(ends_ref[e, HEAD_DIM:, :], hm)
        new = sum(mm(p, pbd) for p in halves(s)) + ends_ref[e, :HEAD_DIM, :].astype(f32)
        return jnp.where(e < place, new, s)

    s = lax.fori_loop(0, devices - 1, hop, jnp.zeros((HEAD_DIM, lanes), f32), unroll=True)
    sbd = spread(s.astype(bf16), hm)
    gain = gain_ref[...]
    for j, (local_ref, reach_ref) in enumerate(zip(refs[:parts], refs[parts : 2 * parts])):
        rows = local_ref.shape[0]
        at = pl.ds(j * rows, rows)
        head_out = local_ref[...] + mm(reach_ref[...], sbd, NT)
        centred = head_out - exact_right(head_out, ones_bd, halves) * (1.0 / HEAD_DIM)
        var = exact_right(centred * centred, ones_bd, halves) * (1.0 / HEAD_DIM)
        gate = jax.nn.sigmoid(gate_ref[at, :].astype(f32))
        mixed_s[at, :] = centred * lax.rsqrt(var + group_eps) * gain * gate
    count, rows, _ = out_ref.shape
    for m in range(count):
        at = pl.multiple_of(lax.bitwise_xor(place_ref[0], m) * rows, rows)
        out_ref[m] = mixed_s[pl.ds(at, rows), :].astype(bf16)


def whole(shape):
    return pl.BlockSpec(shape, lambda i: (0,) * len(shape))


def mixer_finish(place, ends, gate, gain, local, reach, count):
    rows, lanes = gate.shape
    gain = gain.reshape(1, -1)
    out = (count, rows // count, lanes)
    return pl.pallas_call(
        finish_kernel,
        grid=(1,),
        out_shape=jax.ShapeDtypeStruct(out, bf16),
        in_specs=[pl.BlockSpec(memory_space=pltpu.SMEM)]
        + [whole(x.shape) for x in (ends, gate, gain, *local, *reach)],
        out_specs=whole(out),
        scratch_shapes=[pltpu.VMEM(gate.shape, f32)],
        compiler_params=pltpu.CompilerParams(vmem_limit_bytes=VMEM_LIMIT),
        cost_estimate=pl.CostEstimate(flops=4_000_000_000, bytes_accessed=2_000_000, transcendentals=0),
        name="mixer_finish",
    )(place, *hbm(ends, gate, gain, *local, *reach))


def route_kernel(place_ref, x_ref, gain_ref, gw_ref, ew_ref, routes_ref, *outs):
    send_refs, info_ref = outs[:-1], outs[-1]
    tokens, _ = x_ref.shape
    experts, part, share = send_refs[0].shape
    per_group = experts // GROUPS
    x = x_ref[...].astype(f32)
    scale = lax.rsqrt(jnp.mean(x * x, axis=-1, keepdims=True) + norm_eps)
    normed = (x * scale * gain_ref[...]).astype(bf16)
    group_exp = jnp.exp(mm(gw_ref[...], normed, NT))
    group_prob = group_exp / jnp.sum(group_exp, axis=0, keepdims=True)
    logit = mm(ew_ref[...], normed, NT)
    top = routes_ref.shape[0]
    ids = [routes_ref[k : k + 1, :] for k in range(top)]
    match = [iota((experts, tokens), 0) == i for i in ids]
    chosen = [jnp.sum(jnp.where(m, logit, 0.0), axis=0, keepdims=True) for m in match]
    group = [
        jnp.sum(
            jnp.where(iota((GROUPS, tokens), 0) == i // per_group, group_prob, 0.0),
            axis=0, keepdims=True,
        )
        for i in ids
    ]
    weights = [group[k] * jax.nn.sigmoid(chosen[k] - chosen[top - 1 - k]) for k in range(top)]
    counts = sum(m.astype(f32) for m in match)
    earlier = (iota((tokens, tokens), 0) < iota((tokens, tokens), 1)).astype(bf16)
    before = mm(counts.astype(bf16), earlier)
    placed = [jnp.sum(jnp.where(m, before, 0.0), axis=0, keepdims=True) for m in match]
    rows = weights + placed + [i.astype(f32) for i in ids]
    rows += [jnp.zeros((1, tokens), f32)] * (8 - len(rows))
    info_ref[...] = jnp.transpose(jnp.concatenate(rows, axis=0))
    own = pl.multiple_of(place_ref[0] * share, share)
    mine = (
        x_ref[:, pl.ds(own, share)].astype(f32) * scale * gain_ref[:, pl.ds(own, share)]
    ).astype(bf16)
    slots = iota((experts * part, tokens), 0)
    for j, send_ref in enumerate(send_refs):
        hit = None
        for i, p in zip(ids, placed):
            p = p.astype(jnp.int32)
            inside = jnp.logical_and(p >= j * part, p < (j + 1) * part)
            h = jnp.logical_and(slots == i * part + p - j * part, inside)
            hit = h if hit is None else jnp.logical_or(hit, h)
        send_ref[...] = mm(hit.astype(bf16), mine).astype(bf16).reshape(experts, part, share)


def route(place, x, gain, gw, ew, routes, parts, part, share):
    experts, tokens = ew.shape[0], x.shape[0]
    gain = gain.reshape(1, -1)
    return pl.pallas_call(
        route_kernel,
        grid=(1,),
        out_shape=[pltpu.HBM((experts, part, share), bf16)] * parts + [pltpu.HBM((tokens, 8), f32)],
        in_specs=[pl.BlockSpec(memory_space=pltpu.SMEM)]
        + [whole(a.shape) for a in (x, gain, gw, ew, routes)],
        out_specs=[whole((experts, part, share))] * parts + [whole((tokens, 8))],
        compiler_params=pltpu.CompilerParams(vmem_limit_bytes=VMEM_LIMIT),
        cost_estimate=pl.CostEstimate(flops=4_000_000_000, bytes_accessed=1_000_000, transcendentals=0),
        name="route",
    )(place, *hbm(x, gain, gw, ew, routes))


def combine_kernel(place_ref, info_ref, *refs, top):
    homes, out_ref, home_s = refs[:-2], refs[-2], refs[-1]
    tokens = info_ref.shape[0]
    part, share = homes[0].shape
    for j, home in enumerate(homes):
        home_s[j * part : (j + 1) * part, :] = home[...]
    home = home_s[...]
    slots = iota((tokens, home.shape[0]), 1)
    total = jnp.zeros((tokens, share), f32)
    for k in range(top):
        p = info_ref[:, top + k : top + k + 1].astype(jnp.int32)
        i = info_ref[:, 2 * top + k : 2 * top + k + 1].astype(jnp.int32)
        hit = slots == lax.bitwise_xor(i, place_ref[1]) * part + p
        total += info_ref[:, k : k + 1] * mm(hit.astype(bf16), home)
    out_ref[...] = total.astype(bf16)


def combine(place, info, homes, top):
    part, share = homes[0].shape
    out = (info.shape[0], share)
    vm = pl.BlockSpec(memory_space=pltpu.VMEM)
    return pl.pallas_call(
        functools.partial(combine_kernel, top=top),
        out_shape=jax.ShapeDtypeStruct(out, bf16),
        in_specs=[pl.BlockSpec(memory_space=pltpu.SMEM)] + [vm] * (1 + len(homes)),
        out_specs=vm,
        scratch_shapes=[pltpu.VMEM((part * len(homes), share), bf16)],
        compiler_params=pltpu.CompilerParams(vmem_limit_bytes=VMEM_LIMIT),
        cost_estimate=pl.CostEstimate(flops=1_000_000_000, bytes_accessed=1_000_000, transcendentals=0),
        name="combine",
    )(place, info, *homes)


def merge_kernel(keep_ref, got_ref, *outs, offset):
    part = outs[0].shape[0]
    for j, out_ref in enumerate(outs):
        at = j * part
        total = keep_ref[0, offset + at : offset + at + part, :].astype(f32)
        total += got_ref[0, at : at + part, :].astype(f32)
        out_ref[...] = total.astype(bf16)


def merge(keep, got, offset, part):
    _, rows, share = got.shape
    vm = pl.BlockSpec(memory_space=pltpu.VMEM)
    return pl.pallas_call(
        functools.partial(merge_kernel, offset=offset),
        out_shape=[jax.ShapeDtypeStruct((part, share), bf16)] * (rows // part),
        in_specs=[vm] * 2,
        out_specs=[vm] * (rows // part),
        compiler_params=pltpu.CompilerParams(vmem_limit_bytes=VMEM_LIMIT),
        cost_estimate=pl.CostEstimate(flops=100_000_000, bytes_accessed=1_000_000, transcendentals=0),
        name="merge",
    )(keep, got)


def split_kernel(keep_ref, got_ref, keep_out, *outs):
    blocks, rows, _ = keep_out.shape
    half = rows // len(outs)
    for j in range(blocks):
        mine = keep_ref[2 * j].astype(f32) + got_ref[2 * j].astype(f32)
        keep_out[j] = mine.astype(bf16)
        away = (keep_ref[2 * j + 1].astype(f32) + got_ref[2 * j + 1].astype(f32)).astype(bf16)
        for n, out_ref in enumerate(outs):
            out_ref[j] = away[n * half : (n + 1) * half]


def split(keep, got, pieces):
    blocks, rows, share = keep.shape
    vm = pl.BlockSpec(memory_space=pltpu.VMEM)
    return pl.pallas_call(
        split_kernel,
        out_shape=[jax.ShapeDtypeStruct((blocks // 2, rows, share), bf16)]
        + [jax.ShapeDtypeStruct((blocks // 2, rows // pieces, share), bf16)] * pieces,
        in_specs=[vm] * 2,
        out_specs=[vm] * (1 + pieces),
        compiler_params=pltpu.CompilerParams(vmem_limit_bytes=VMEM_LIMIT),
        cost_estimate=pl.CostEstimate(flops=100_000_000, bytes_accessed=1_000_000, transcendentals=0),
        name="split",
    )(keep, got)


def tile_of(size, most):
    return most if size % most == 0 else size


def experts_kernel(place_ref, *refs, masks, sends, sources):
    count = len(masks)
    xs = refs[:count]
    wg_hbm, wu_hbm, wd_hbm, h_ref, send_ref, wg, wu, wd, gate_sem, down_sem = refs[count:]
    rows, share = xs[0].shape
    tiles, _, _, tile = wg.shape

    def rows_of(m):
        return pl.ds(pl.multiple_of(lax.bitwise_xor(place_ref[0], m) * share, share), share)

    loads = {}
    for f in range(tiles):
        for n, m in enumerate(masks):
            columns = pl.ds(f * tile, tile)
            loads[f, n] = [
                pltpu.make_async_copy(
                    src.at[0, rows_of(m), columns], dst.at[f, n], gate_sem.at[i, f, n]
                )
                for i, (src, dst) in enumerate(((wg_hbm, wg), (wu_hbm, wu)))
            ]
            for load in loads[f, n]:
                load.start()
    downs = [
        pltpu.make_async_copy(wd_hbm.at[0, :, rows_of(m)], wd.at[n], down_sem.at[n])
        for n, m in enumerate(sends)
    ]
    for load in downs:
        load.start()
    for f in range(tiles):
        gate = up = None
        for n, x in enumerate(xs):
            for load in loads[f, n]:
                load.wait()
            x = x[...]
            g, u = mm(x, wg[f, n]), mm(x, wu[f, n])
            gate, up = (g, u) if gate is None else (gate + g, up + u)
        h = (gate * jax.nn.sigmoid(gate) * up).astype(bf16)
        part = rows // sources
        for s in range(sources):
            at = pl.multiple_of(lax.bitwise_xor(place_ref[1], s) * part, part)
            h_ref[pl.ds(at, part), f * tile : (f + 1) * tile] = h[s * part : (s + 1) * part]
    h = h_ref[...]
    for n, load in enumerate(downs):
        load.wait()
        send_ref[n] = mm(h, wd[n]).astype(bf16)


def run_experts(place, masks, sends, xs, wg, wu, wd, sources):
    rows, share = xs[0].shape
    _, width, units = wg.shape
    tile = tile_of(units, 256)
    tiles = units // tile
    vm = pl.BlockSpec(memory_space=pltpu.VMEM)
    held = pltpu.VMEM((tiles, len(masks), share, tile), bf16)
    return pl.pallas_call(
        functools.partial(experts_kernel, masks=masks, sends=tuple(sends), sources=sources),
        in_specs=[pl.BlockSpec(memory_space=pltpu.SMEM)]
        + [vm] * len(xs)
        + [pl.BlockSpec(memory_space=pltpu.HBM)] * 3,
        out_specs=[vm] * 2,
        out_shape=[
            jax.ShapeDtypeStruct((rows, units), bf16),
            jax.ShapeDtypeStruct((len(sends), rows, share), bf16),
        ],
        scratch_shapes=[
            held, held, pltpu.VMEM((len(sends), units, share), bf16),
            pltpu.SemaphoreType.DMA((2, tiles, len(masks))), pltpu.SemaphoreType.DMA((len(sends),)),
        ],
        compiler_params=pltpu.CompilerParams(vmem_limit_bytes=VMEM_LIMIT),
        cost_estimate=pl.CostEstimate(
            flops=4 * rows * width * units, bytes_accessed=4 * width * units, transcendentals=0
        ),
        name="experts",
    )(place, *xs, *hbm(wg, wu, wd))


def keep_kernel(place_ref, h_ref, w_ref, out_ref):
    out_ref[0] = mm(h_ref[...], w_ref[0]).astype(bf16)


def keep_down(place, masks, h, wd, share):
    rows, units = h.shape
    masks = tuple(masks)

    def column(i, p):
        mask = jnp.int32(masks[-1])
        for j in range(len(masks) - 2, -1, -1):
            mask = jnp.where(i == j, jnp.int32(masks[j]), mask)
        return 0, 0, lax.bitwise_xor(p[0], mask)

    return pl.pallas_call(
        keep_kernel,
        grid_spec=pltpu.PrefetchScalarGridSpec(
            num_scalar_prefetch=1,
            grid=(len(masks),),
            in_specs=[
                pl.BlockSpec((rows, units), lambda i, p: (0, 0)),
                pl.BlockSpec((1, units, share), column),
            ],
            out_specs=pl.BlockSpec((1, rows, share), lambda i, p: (i, 0, 0)),
        ),
        out_shape=jax.ShapeDtypeStruct((len(masks), rows, share), bf16),
        compiler_params=pltpu.CompilerParams(vmem_limit_bytes=VMEM_LIMIT),
        cost_estimate=pl.CostEstimate(
            flops=2 * rows * units * share * len(masks),
            bytes_accessed=2 * units * share * len(masks), transcendentals=0,
        ),
        name="keep_down",
    )(place, h, *hbm(wd))


def project_kernel(*refs):
    out_ref = refs[-1]
    count = (len(refs) - 1) // 2
    total = None
    for x, w in zip(refs[:count], refs[count:-1]):
        p = mm(x[...], w[...]).astype(bf16).astype(f32)
        total = p if total is None else total + p
    out_ref[...] = total.astype(bf16)


def project(xs, ws):
    rows, lanes = xs[0].shape
    width = ws[0].shape[1]
    tile = tile_of(width, 512)
    return pl.pallas_call(
        project_kernel,
        grid=(width // tile,),
        in_specs=[pl.BlockSpec((rows, lanes), lambda i: (0, 0))] * len(xs)
        + [pl.BlockSpec((lanes, tile), lambda i: (0, i))] * len(ws),
        out_specs=pl.BlockSpec((rows, tile), lambda i: (0, i)),
        out_shape=jax.ShapeDtypeStruct((rows, width), bf16),
        compiler_params=pltpu.CompilerParams(vmem_limit_bytes=VMEM_LIMIT),
        cost_estimate=pl.CostEstimate(
            flops=2 * rows * lanes * width * len(xs),
            bytes_accessed=2 * lanes * width * len(xs), transcendentals=0,
        ),
        name="project",
    )(*xs, *ws)


def swap(x, mask):
    count = lax.axis_size("tp")
    return lax.ppermute(x, "tp", [(i, i ^ mask) for i in range(count)])


def hop(x, mask):
    count = lax.axis_size("ep")
    return lax.ppermute(x, "ep", [(i, i ^ mask) for i in range(count)])


def gathered(x, far=None):
    masks, blocks = [0], [x]
    mask = lax.axis_size("tp") // 2
    if far is not None:
        masks, blocks, mask = [0, mask], [x, far], mask // 2
    while mask:
        more = []
        for b in blocks:
            more.append(swap(b, mask))
        blocks += more
        masks += [m ^ mask for m in masks]
        mask //= 2
    return tuple(masks), blocks


def local(
    receptance, key_matrix, value_matrix, decay_data_term, correction_rate_data,
    output_gate_input, decay_channel_offset, correction_rate_offset, extra_head_log_decay,
    head_norm_gain, mixer_output_weight, expert_layer_input, feedforward_norm_gain,
    group_router_weight, expert_router_weight, routes, expert_gate_weight, expert_up_weight,
    expert_down_weight,
):
    ep, tp = lax.axis_size("ep"), lax.axis_size("tp")
    place = lax.axis_index("tp").reshape(1).astype(jnp.int32)
    turn = lax.axis_index("ep").reshape(1).astype(jnp.int32)
    both = jnp.concatenate([place, turn])
    tokens, width = expert_layer_input.shape
    experts = expert_router_weight.shape[1]
    share = width // tp
    capacity = 4 * tokens // ep

    weight_far = swap(mixer_output_weight, tp // 2)
    send, info = route(
        place, expert_layer_input, feedforward_norm_gain, group_router_weight.T,
        expert_router_weight.T, routes.T, 1, capacity, share,
    )
    arrived = lax.all_to_all(send, "ep", split_axis=0, concat_axis=0, tiled=True)

    mixer_args = (
        receptance, key_matrix, value_matrix, decay_data_term, correction_rate_data,
        decay_channel_offset, correction_rate_offset, extra_head_log_decay.T,
    )
    local_a, reach_a, state = mixer_local(0, 2, ep, None, *mixer_args)
    arrived, state = lax.optimization_barrier((arrived, state))
    rows_in = arrived.reshape(experts * capacity, share)
    far = swap(rows_in, tp // 2)
    local_b, reach_b, end = mixer_local(1, 2, ep, state, *mixer_args)
    far, weight_far, local_b = lax.optimization_barrier((far, weight_far, local_b))
    weight_masks, weight_blocks = gathered(mixer_output_weight, weight_far)
    ends = lax.all_to_all(end, "ep", split_axis=0, concat_axis=0, tiled=True)

    masks, blocks = gathered(rows_in, far)
    odd = [m for m in range(tp) if m & 1]
    even = [m for m in range(tp) if not m & 1]
    h, send = run_experts(
        both, masks, odd, blocks, expert_gate_weight, expert_up_weight, expert_down_weight, ep
    )
    keep = keep_down(place, even, h, expert_down_weight, share)
    bit = 1
    got = swap(send, bit)
    while 2 * bit < tp:
        bit *= 2
        if 2 * bit < tp:
            keep, send = split(keep, got, 1)
            got = swap(send, bit)
        else:
            keep, near, away = split(keep, got, 2)
    half = near.shape[1]
    away = swap(away, bit)
    near = swap(near, bit)
    away = merge(keep, away, half, capacity)
    away = [hop(x, ep // 2 + m) for m, x in enumerate(away)]
    near = merge(keep, near, 0, capacity)
    near = [near[0]] + [hop(x, m) for m, x in enumerate(near) if m]
    homes = near + away

    mixed = mixer_finish(
        both, ends, output_gate_input, head_norm_gain,
        (local_a, local_b), (reach_a, reach_b), tp,
    )
    pieces = [mixed[m] if m == 0 else swap(mixed[m], m) for m in weight_masks]
    token_mixer_output = project(pieces, weight_blocks)
    expert_out = combine(both, info, homes, routes.shape[1])
    return (token_mixer_output, expert_out)


def solution(mesh):
    in_specs = (
        P("ep", "tp"), P("ep", "tp"), P("ep", "tp"), P("ep", "tp"), P("ep", "tp"), P("ep", "tp"),
        P("tp"), P("tp"), P("ep", "tp"), P("tp"), P("tp", None), P("ep", None), P(), P(), P(),
        P("ep", None), P("ep", None, "tp"), P("ep", None, "tp"), P("ep", "tp", None),
    )
    out_specs = (P(("ep", "tp"), None), P("ep", "tp"))
    return jax.shard_map(local, mesh=mesh, in_specs=in_specs, out_specs=out_specs, check_vma=False)
```

```python
import functools
import jax
import jax.numpy as jnp
from jax import lax
from jax.experimental import pallas as pl
from jax.experimental.pallas import tpu as pltpu
from jax.sharding import PartitionSpec as P

HEAD_DIM = 64
GROUPS = 4
VMEM_LIMIT = 16 * 1024 * 1024
key_eps = 1e-06
group_eps = 0.00064
norm_eps = 1e-06
BASE = 16

f32, bf16 = jnp.float32, jnp.bfloat16
NN = (((1,), (0,)), ((), ()))
NT = (((1,), (1,)), ((), ()))
TN = (((0,), (0,)), ((), ()))


def hbm(*arrays):
    return [pltpu.with_memory_space_constraint(a, pltpu.HBM) for a in arrays]


def mm(a, b, dims=NN):
    return lax.dot_general(a, b, dims, preferred_element_type=f32)


def halves(x):
    high = x.astype(bf16)
    return high, (x - high.astype(f32)).astype(bf16)


def thirds(x):
    high = x.astype(bf16)
    rest = x - high.astype(f32)
    mid = rest.astype(bf16)
    return high, mid, (rest - mid.astype(f32)).astype(bf16)


def exact_right(x, ones, parts):
    return sum(mm(p, ones) for p in parts(x))


def exact_left(ones, x, parts):
    return sum(mm(ones, p) for p in parts(x))


def iota(shape, axis):
    return lax.broadcasted_iota(jnp.int32, shape, axis)


def head_mask(lanes):
    return iota((lanes, lanes), 0) // HEAD_DIM == iota((lanes, lanes), 1) // HEAD_DIM


def spread(x, mask):
    rep = mask.shape[0] // HEAD_DIM
    return jnp.where(mask, jnp.concatenate([x] * rep, axis=0), jnp.zeros((), x.dtype))


def fold(x):
    pieces = [x[i : i + HEAD_DIM] for i in range(0, x.shape[0], HEAD_DIM)]
    return functools.reduce(jnp.add, pieces)


def mixer_kernel(
    base, first_part, last_part, q_in, k_in, v_in, w_in, a_in, wo_ref, ao_ref, ex_ref, *refs
):
    refs = list(refs)
    *refs, q_ref, k_ref, v_ref, w_ref, a_ref, in_sem = refs
    loads = [
        pltpu.make_async_copy(src.at[pl.ds(base, dst.shape[0]), :], dst, in_sem.at[n])
        for n, (src, dst) in enumerate(
            ((k_in, k_ref), (a_in, a_ref), (w_in, w_ref), (q_in, q_ref), (v_in, v_ref))
        )
    ]
    for load in loads:
        load.start()
    for load in loads:
        load.wait()
    start_ref = None if first_part else refs.pop(0)
    local_ref, reach_ref, end_ref = refs[:3]
    (
        u_s, r_s, ld_s, pair_s, diag_s, tri_s, ue_s, qe_s, kh_s, rh_s, up_s, qp_s, g_s, et_s,
    ) = refs[3:]
    rows, lanes = q_ref.shape
    C = HEAD_DIM
    chunks = rows // C
    heads = lanes // HEAD_DIM
    hm = head_mask(lanes)
    ones_bd = hm.astype(bf16)

    k = k_ref[...].astype(f32)
    u = k * lax.rsqrt(exact_right(k * k, ones_bd, halves) + key_eps)
    u_s[...] = u
    r_s[...] = u * jax.nn.sigmoid(a_ref[...].astype(f32) + ao_ref[...])
    owner = (iota((heads, lanes), 1) // HEAD_DIM == iota((heads, lanes), 0)).astype(bf16)
    exb = sum(mm(p, owner, TN) for p in thirds(ex_ref[...]))[base : base + rows]
    pre = w_ref[...].astype(f32) + wo_ref[...]
    ld_s[...] = exb - jax.nn.sigmoid(pre) * 0.6065306597126334

    tri = (iota((C, C), 0) >= iota((C, C), 1)).astype(bf16)
    same = head_mask(lanes)
    rr, cc = iota((lanes, lanes), 0), iota((lanes, lanes), 1)
    strict = jnp.logical_and(same, rr > cc)
    upto = jnp.logical_and(same, rr >= cc)
    base_mask = rr // BASE == cc // BASE

    def first(i, _):
        at = pl.ds(pl.multiple_of(i * C, C), C)
        ld = ld_s[at, :]
        c = exact_left(tri, ld, thirds)
        tot = c[C - 1 : C, :]
        mid = 0.5 * tot
        em = jnp.exp(mid)
        eq = jnp.exp(c - mid)
        eu = jnp.exp(c - ld - mid)
        ek = jnp.exp(mid - c)
        ut, qt = u_s[at, :] * eu, q_ref[at, :].astype(f32) * eq
        kt, rt = k_ref[at, :].astype(f32) * ek, r_s[at, :] * ek
        ue_s[at, :] = (ut * em).astype(bf16)
        qe_s[at, :] = qt * em
        kh_s[at, :] = (kt * em).astype(bf16)
        rh_s[at, :] = (rt * em).astype(bf16)
        et_s[pl.ds(i, 1), :] = em * em
        left = jnp.concatenate([spread(ut.astype(bf16), hm), spread(qt.astype(bf16), hm)], axis=0)
        right = jnp.concatenate([spread(kt.astype(bf16), hm), spread(rt.astype(bf16), hm)], axis=0)
        pairs = mm(left, right, NT)
        uk = jnp.where(strict, pairs[:lanes, :lanes], 0.0)
        ur = jnp.where(strict, pairs[:lanes, lanes:], 0.0)
        qk = jnp.where(upto, pairs[lanes:, :lanes], 0.0)
        qr = jnp.where(upto, pairs[lanes:, lanes:], 0.0)
        pair_s[i, 0] = uk.astype(bf16)
        pair_s[i, 1] = ur.astype(bf16)
        pair_s[i, 2] = qk.astype(bf16)
        pair_s[i, 3] = qr.astype(bf16)
        dg = jnp.where(base_mask, ur, 0.0)
        diag_s[i] = functools.reduce(
            jnp.add, [dg[p : p + BASE] for p in range(0, lanes, BASE)]
        )
        return 0

    lax.fori_loop(0, chunks, first, 0, unroll=True)

    dall = diag_s[...].reshape(chunks * BASE, lanes)
    dparts = thirds(dall)
    t = jnp.where(
        iota((chunks, BASE, lanes), 1) == iota((chunks, BASE, lanes), 2) % BASE, 1.0, 0.0
    ).astype(f32)
    for j in range(BASE - 1):
        if lanes % 128:
            pick = jnp.logical_and(base_mask, rr % BASE == j).astype(bf16)
            col = sum(mm(p, pick) for p in dparts)
        else:
            near = iota((chunks * BASE, 128), 1) // BASE * BASE + j
            col = jnp.concatenate(
                [
                    jnp.take_along_axis(dall[:, p : p + 128], near, axis=1, mode="promise_in_bounds")
                    for p in range(0, lanes, 128)
                ],
                axis=1,
            )
        col = col.reshape(chunks, BASE, lanes)
        t = t - col * t[:, j : j + 1, :]
    tri_s[...] = t

    m32 = jnp.logical_and(rr // (2 * BASE) == cc // (2 * BASE), jnp.logical_not(base_mask))
    m64 = rr // (2 * BASE) != cc // (2 * BASE)
    pickv = (iota((HEAD_DIM, lanes), 0) == iota((HEAD_DIM, lanes), 1) % HEAD_DIM).astype(bf16)
    zero = jnp.zeros((), bf16)

    def second(i, _):
        at = pl.ds(pl.multiple_of(i * C, C), C)
        uk, ur, qk, qr = pair_s[i, 0], pair_s[i, 1], pair_s[i, 2], pair_s[i, 3]
        td = tri_s[i]
        t16 = jnp.where(base_mask, jnp.concatenate([td] * (lanes // BASE), axis=0), 0.0)
        t16b = t16.astype(bf16)
        p1 = mm(jnp.where(m32, ur, zero), t16b).astype(bf16)
        t32 = t16 - mm(t16b, p1)
        t32b = t32.astype(bf16)
        p2 = mm(jnp.where(m64, ur, zero), t32b).astype(bf16)
        t64 = (t32 - mm(t32b, p2)).astype(bf16)
        ubd = spread(ue_s[at, :], hm)
        ta = mm(t64, uk).astype(bf16)
        up = mm(t64, ubd).astype(bf16)
        up_s[i] = up
        vbd = spread(v_ref[at, :], hm)
        za = mm(ta, vbd)
        o = mm(qk, vbd) - mm(qr, za.astype(bf16))
        local_ref[at, :] = fold(o)
        qp_s[at, :] = (qe_s[at, :] - fold(mm(qr, up))).astype(bf16)
        vt = mm(pickv, vbd, NT).astype(bf16)
        zat = mm(vt, ta, NT).astype(bf16)
        g_s[i] = mm(vt, spread(kh_s[at, :], hm)) - mm(zat, spread(rh_s[at, :], hm))
        return 0

    lax.fori_loop(0, chunks, second, 0, unroll=True)

    def third(i, x):
        at = pl.ds(pl.multiple_of(i * C, C), C)
        xb = x.astype(bf16)
        xs, xm = xb[:HEAD_DIM], xb[HEAD_DIM:]
        qp = qp_s[at, :]
        local_ref[at, :] += mm(qp, spread(xs, hm), NT)
        reach_ref[at, :] = mm(qp, spread(xm, hm), NT).astype(bf16)
        at_ = mm(xb, up_s[i], NT).astype(bf16)
        corr = mm(at_, spread(rh_s[at, :], hm))
        g = g_s[i]
        return x * et_s[pl.ds(i, 1), :] + jnp.concatenate([g, jnp.zeros_like(g)], axis=0) - corr

    if first_part:
        x0 = jnp.concatenate([jnp.zeros((HEAD_DIM, lanes), f32), pickv.astype(f32)], axis=0)
    else:
        x0 = start_ref[...]
    x = lax.fori_loop(0, chunks, third, x0, unroll=True)
    if last_part:
        end_ref[...] = jnp.broadcast_to(x.astype(bf16)[None], end_ref.shape)
    else:
        end_ref[...] = x


def mixer_local(part, copies, start, q, k, v, w, a, wo, ao, ex):
    total, lanes = q.shape
    cut = -(-(total // HEAD_DIM) * 5 // 8)
    base, chunks = ((0, cut), (cut, total // HEAD_DIM - cut))[part]
    base, rows = base * HEAD_DIM, chunks * HEAD_DIM
    heads = ex.shape[0]
    V = pltpu.VMEM
    vector = pl.BlockSpec((1, lanes), lambda i: (0, 0))
    state = pl.BlockSpec((2 * HEAD_DIM, lanes), lambda i: (0, 0))
    out = pl.BlockSpec((rows, lanes), lambda i: (0, 0))
    last = part == 1
    ends = (copies, 2 * HEAD_DIM, lanes)
    return pl.pallas_call(
        functools.partial(mixer_kernel, base, part == 0, last),
        grid=(1,),
        in_specs=[pl.BlockSpec(memory_space=pltpu.HBM)] * 5
        + [vector] * 2
        + [pl.BlockSpec((heads, total), lambda i: (0, 0))]
        + ([] if start is None else [state]),
        out_specs=[out, out, pl.BlockSpec(ends, lambda i: (0, 0, 0)) if last else state],
        out_shape=[
            pltpu.HBM((rows, lanes), f32),
            pltpu.HBM((rows, lanes), bf16),
            pltpu.HBM(ends, bf16) if last else jax.ShapeDtypeStruct(ends[1:], f32),
        ],
        scratch_shapes=[
            V((rows, lanes), f32), V((rows, lanes), f32), V((rows, lanes), f32),
            V((chunks, 4, lanes, lanes), bf16), V((chunks, BASE, lanes), f32), V((chunks, BASE, lanes), f32),
            V((rows, lanes), bf16), V((rows, lanes), f32), V((rows, lanes), bf16), V((rows, lanes), bf16),
            V((chunks, lanes, lanes), bf16), V((rows, lanes), bf16), V((chunks, HEAD_DIM, lanes), f32),
            V((chunks, lanes), f32),
        ]
        + [V((rows, lanes), bf16)] * 5
        + [pltpu.SemaphoreType.DMA((5,))],
        compiler_params=pltpu.CompilerParams(vmem_limit_bytes=VMEM_LIMIT),
        cost_estimate=pl.CostEstimate(flops=10_000_000_000, bytes_accessed=2_000_000, transcendentals=0),
        name="mixer_local",
    )(
        *hbm(q, k, v, w, a, wo.reshape(1, -1), ao.reshape(1, -1), ex),
        *([] if start is None else [start]),
    )


def finish_kernel(place_ref, ends_ref, gate_ref, gain_ref, *refs):
    out_ref, mixed_s = refs[-2:]
    parts = (len(refs) - 2) // 2
    devices, _, lanes = ends_ref.shape
    hm = head_mask(lanes)
    ones_bd = hm.astype(bf16)
    place = place_ref[1]

    def hop(e, s):
        pbd = spread(ends_ref[e, HEAD_DIM:, :], hm)
        new = sum(mm(p, pbd) for p in halves(s)) + ends_ref[e, :HEAD_DIM, :].astype(f32)
        return jnp.where(e < place, new, s)

    s = lax.fori_loop(0, devices - 1, hop, jnp.zeros((HEAD_DIM, lanes), f32), unroll=True)
    sbd = spread(s.astype(bf16), hm)
    gain, begin = gain_ref[...], 0
    for local_ref, reach_ref in zip(refs[:parts], refs[parts : 2 * parts]):
        rows = local_ref.shape[0]
        at = pl.ds(begin, rows)
        begin += rows
        head_out = local_ref[...] + mm(reach_ref[...], sbd, NT)
        centred = head_out - exact_right(head_out, ones_bd, halves) * (1.0 / HEAD_DIM)
        var = exact_right(centred * centred, ones_bd, halves) * (1.0 / HEAD_DIM)
        gate = jax.nn.sigmoid(gate_ref[at, :].astype(f32))
        mixed_s[at, :] = centred * lax.rsqrt(var + group_eps) * gain * gate
    count, rows, _ = out_ref.shape
    for m in range(count):
        at = pl.multiple_of(lax.bitwise_xor(place_ref[0], m) * rows, rows)
        out_ref[m] = mixed_s[pl.ds(at, rows), :].astype(bf16)


def whole(shape):
    return pl.BlockSpec(shape, lambda i: (0,) * len(shape))


def mixer_finish(place, ends, gate, gain, local, reach, count):
    rows, lanes = gate.shape
    gain = gain.reshape(1, -1)
    out = (count, rows // count, lanes)
    return pl.pallas_call(
        finish_kernel,
        grid=(1,),
        out_shape=jax.ShapeDtypeStruct(out, bf16),
        in_specs=[pl.BlockSpec(memory_space=pltpu.SMEM)]
        + [whole(x.shape) for x in (ends, gate, gain, *local, *reach)],
        out_specs=whole(out),
        scratch_shapes=[pltpu.VMEM(gate.shape, f32)],
        compiler_params=pltpu.CompilerParams(vmem_limit_bytes=VMEM_LIMIT),
        cost_estimate=pl.CostEstimate(flops=4_000_000_000, bytes_accessed=2_000_000, transcendentals=0),
        name="mixer_finish",
    )(place, *hbm(ends, gate, gain, *local, *reach))


def route_kernel(place_ref, x_ref, gain_ref, gw_ref, ew_ref, routes_ref, *outs):
    send_refs, info_ref = outs[:-1], outs[-1]
    tokens, _ = x_ref.shape
    experts, part, share = send_refs[0].shape
    per_group = experts // GROUPS
    x = x_ref[...].astype(f32)
    scale = lax.rsqrt(jnp.mean(x * x, axis=-1, keepdims=True) + norm_eps)
    normed = (x * scale * gain_ref[...]).astype(bf16)
    group_exp = jnp.exp(mm(gw_ref[...], normed, NT))
    group_prob = group_exp / jnp.sum(group_exp, axis=0, keepdims=True)
    logit = mm(ew_ref[...], normed, NT)
    top = routes_ref.shape[0]
    ids = [routes_ref[k : k + 1, :] for k in range(top)]
    match = [iota((experts, tokens), 0) == i for i in ids]
    chosen = [jnp.sum(jnp.where(m, logit, 0.0), axis=0, keepdims=True) for m in match]
    group = [
        jnp.sum(
            jnp.where(iota((GROUPS, tokens), 0) == i // per_group, group_prob, 0.0),
            axis=0, keepdims=True,
        )
        for i in ids
    ]
    weights = [group[k] * jax.nn.sigmoid(chosen[k] - chosen[top - 1 - k]) for k in range(top)]
    counts = sum(m.astype(f32) for m in match)
    earlier = (iota((tokens, tokens), 0) < iota((tokens, tokens), 1)).astype(bf16)
    before = mm(counts.astype(bf16), earlier)
    placed = [jnp.sum(jnp.where(m, before, 0.0), axis=0, keepdims=True) for m in match]
    rows = weights + placed + [i.astype(f32) for i in ids]
    rows += [jnp.zeros((1, tokens), f32)] * (8 - len(rows))
    info_ref[...] = jnp.transpose(jnp.concatenate(rows, axis=0))
    own = pl.multiple_of(place_ref[0] * share, share)
    mine = (
        x_ref[:, pl.ds(own, share)].astype(f32) * scale * gain_ref[:, pl.ds(own, share)]
    ).astype(bf16)
    slots = iota((experts * part, tokens), 0)
    for j, send_ref in enumerate(send_refs):
        hit = None
        for i, p in zip(ids, placed):
            p = p.astype(jnp.int32)
            inside = jnp.logical_and(p >= j * part, p < (j + 1) * part)
            h = jnp.logical_and(slots == i * part + p - j * part, inside)
            hit = h if hit is None else jnp.logical_or(hit, h)
        send_ref[...] = mm(hit.astype(bf16), mine).astype(bf16).reshape(experts, part, share)


def route(place, x, gain, gw, ew, routes, parts, part, share):
    experts, tokens = ew.shape[0], x.shape[0]
    gain = gain.reshape(1, -1)
    return pl.pallas_call(
        route_kernel,
        grid=(1,),
        out_shape=[pltpu.HBM((experts, part, share), bf16)] * parts + [pltpu.HBM((tokens, 8), f32)],
        in_specs=[pl.BlockSpec(memory_space=pltpu.SMEM)]
        + [whole(a.shape) for a in (x, gain, gw, ew, routes)],
        out_specs=[whole((experts, part, share))] * parts + [whole((tokens, 8))],
        compiler_params=pltpu.CompilerParams(vmem_limit_bytes=VMEM_LIMIT),
        cost_estimate=pl.CostEstimate(flops=4_000_000_000, bytes_accessed=1_000_000, transcendentals=0),
        name="route",
    )(place, *hbm(x, gain, gw, ew, routes))


def combine_kernel(place_ref, info_ref, *refs, top):
    homes, out_ref, home_s = refs[:-2], refs[-2], refs[-1]
    tokens = info_ref.shape[0]
    part, share = homes[0].shape
    for j, home in enumerate(homes):
        home_s[j * part : (j + 1) * part, :] = home[...]
    home = home_s[...]
    slots = iota((tokens, home.shape[0]), 1)
    total = jnp.zeros((tokens, share), f32)
    for k in range(top):
        p = info_ref[:, top + k : top + k + 1].astype(jnp.int32)
        i = info_ref[:, 2 * top + k : 2 * top + k + 1].astype(jnp.int32)
        hit = slots == lax.bitwise_xor(i, place_ref[1]) * part + p
        total += info_ref[:, k : k + 1] * mm(hit.astype(bf16), home)
    out_ref[...] = total.astype(bf16)


def combine(place, info, homes, top):
    part, share = homes[0].shape
    out = (info.shape[0], share)
    vm = pl.BlockSpec(memory_space=pltpu.VMEM)
    return pl.pallas_call(
        functools.partial(combine_kernel, top=top),
        out_shape=jax.ShapeDtypeStruct(out, bf16),
        in_specs=[pl.BlockSpec(memory_space=pltpu.SMEM)] + [vm] * (1 + len(homes)),
        out_specs=vm,
        scratch_shapes=[pltpu.VMEM((part * len(homes), share), bf16)],
        compiler_params=pltpu.CompilerParams(vmem_limit_bytes=VMEM_LIMIT),
        cost_estimate=pl.CostEstimate(flops=1_000_000_000, bytes_accessed=1_000_000, transcendentals=0),
        name="combine",
    )(place, info, *homes)


def merge_kernel(keep_ref, got_ref, *outs, offset):
    part = outs[0].shape[0]
    for j, out_ref in enumerate(outs):
        at = j * part
        total = keep_ref[0, offset + at : offset + at + part, :].astype(f32)
        total += got_ref[0, at : at + part, :].astype(f32)
        out_ref[...] = total.astype(bf16)


def merge(keep, got, offset, part):
    _, rows, share = got.shape
    vm = pl.BlockSpec(memory_space=pltpu.VMEM)
    return pl.pallas_call(
        functools.partial(merge_kernel, offset=offset),
        out_shape=[jax.ShapeDtypeStruct((part, share), bf16)] * (rows // part),
        in_specs=[vm] * 2,
        out_specs=[vm] * (rows // part),
        compiler_params=pltpu.CompilerParams(vmem_limit_bytes=VMEM_LIMIT),
        cost_estimate=pl.CostEstimate(flops=100_000_000, bytes_accessed=1_000_000, transcendentals=0),
        name="merge",
    )(keep, got)


def split_kernel(keep_ref, got_ref, keep_out, *outs):
    blocks, rows, _ = keep_out.shape
    half = rows // len(outs)
    for j in range(blocks):
        mine = keep_ref[2 * j].astype(f32) + got_ref[2 * j].astype(f32)
        keep_out[j] = mine.astype(bf16)
        away = (keep_ref[2 * j + 1].astype(f32) + got_ref[2 * j + 1].astype(f32)).astype(bf16)
        for n, out_ref in enumerate(outs):
            out_ref[j] = away[n * half : (n + 1) * half]


def split(keep, got, pieces):
    blocks, rows, share = keep.shape
    vm = pl.BlockSpec(memory_space=pltpu.VMEM)
    return pl.pallas_call(
        split_kernel,
        out_shape=[jax.ShapeDtypeStruct((blocks // 2, rows, share), bf16)]
        + [jax.ShapeDtypeStruct((blocks // 2, rows // pieces, share), bf16)] * pieces,
        in_specs=[vm] * 2,
        out_specs=[vm] * (1 + pieces),
        compiler_params=pltpu.CompilerParams(vmem_limit_bytes=VMEM_LIMIT),
        cost_estimate=pl.CostEstimate(flops=100_000_000, bytes_accessed=1_000_000, transcendentals=0),
        name="split",
    )(keep, got)


def tile_of(size, most):
    return most if size % most == 0 else size


def experts_kernel(place_ref, *refs, masks, sends, sources):
    count = len(masks)
    xs = refs[:count]
    wg_hbm, wu_hbm, wd_hbm, h_ref, send_ref, wg, wu, wd, gate_sem, down_sem = refs[count:]
    rows, share = xs[0].shape
    tiles, _, _, tile = wg.shape

    def rows_of(m):
        return pl.ds(pl.multiple_of(lax.bitwise_xor(place_ref[0], m) * share, share), share)

    loads = {}
    for f in range(tiles):
        for n, m in enumerate(masks):
            columns = pl.ds(f * tile, tile)
            loads[f, n] = [
                pltpu.make_async_copy(
                    src.at[0, rows_of(m), columns], dst.at[f, n], gate_sem.at[i, f, n]
                )
                for i, (src, dst) in enumerate(((wg_hbm, wg), (wu_hbm, wu)))
            ]
            for load in loads[f, n]:
                load.start()
    downs = [
        pltpu.make_async_copy(wd_hbm.at[0, :, rows_of(m)], wd.at[n], down_sem.at[n])
        for n, m in enumerate(sends)
    ]
    for load in downs:
        load.start()
    for f in range(tiles):
        gate = up = None
        for n, x in enumerate(xs):
            for load in loads[f, n]:
                load.wait()
            x = x[...]
            g, u = mm(x, wg[f, n]), mm(x, wu[f, n])
            gate, up = (g, u) if gate is None else (gate + g, up + u)
        h = (gate * jax.nn.sigmoid(gate) * up).astype(bf16)
        part = rows // sources
        for s in range(sources):
            at = pl.multiple_of(lax.bitwise_xor(place_ref[1], s) * part, part)
            h_ref[pl.ds(at, part), f * tile : (f + 1) * tile] = h[s * part : (s + 1) * part]
    h = h_ref[...]
    for n, load in enumerate(downs):
        load.wait()
        send_ref[n] = mm(h, wd[n]).astype(bf16)


def run_experts(place, masks, sends, xs, wg, wu, wd, sources):
    rows, share = xs[0].shape
    _, width, units = wg.shape
    tile = tile_of(units, 256)
    tiles = units // tile
    vm = pl.BlockSpec(memory_space=pltpu.VMEM)
    held = pltpu.VMEM((tiles, len(masks), share, tile), bf16)
    return pl.pallas_call(
        functools.partial(experts_kernel, masks=masks, sends=tuple(sends), sources=sources),
        in_specs=[pl.BlockSpec(memory_space=pltpu.SMEM)]
        + [vm] * len(xs)
        + [pl.BlockSpec(memory_space=pltpu.HBM)] * 3,
        out_specs=[vm] * 2,
        out_shape=[
            jax.ShapeDtypeStruct((rows, units), bf16),
            jax.ShapeDtypeStruct((len(sends), rows, share), bf16),
        ],
        scratch_shapes=[
            held, held, pltpu.VMEM((len(sends), units, share), bf16),
            pltpu.SemaphoreType.DMA((2, tiles, len(masks))), pltpu.SemaphoreType.DMA((len(sends),)),
        ],
        compiler_params=pltpu.CompilerParams(vmem_limit_bytes=VMEM_LIMIT),
        cost_estimate=pl.CostEstimate(
            flops=4 * rows * width * units, bytes_accessed=4 * width * units, transcendentals=0
        ),
        name="experts",
    )(place, *xs, *hbm(wg, wu, wd))


def keep_kernel(place_ref, h_ref, w_ref, out_ref):
    out_ref[0] = mm(h_ref[...], w_ref[0]).astype(bf16)


def keep_down(place, masks, h, wd, share):
    rows, units = h.shape
    masks = tuple(masks)

    def column(i, p):
        mask = jnp.int32(masks[-1])
        for j in range(len(masks) - 2, -1, -1):
            mask = jnp.where(i == j, jnp.int32(masks[j]), mask)
        return 0, 0, lax.bitwise_xor(p[0], mask)

    return pl.pallas_call(
        keep_kernel,
        grid_spec=pltpu.PrefetchScalarGridSpec(
            num_scalar_prefetch=1,
            grid=(len(masks),),
            in_specs=[
                pl.BlockSpec((rows, units), lambda i, p: (0, 0)),
                pl.BlockSpec((1, units, share), column),
            ],
            out_specs=pl.BlockSpec((1, rows, share), lambda i, p: (i, 0, 0)),
        ),
        out_shape=jax.ShapeDtypeStruct((len(masks), rows, share), bf16),
        compiler_params=pltpu.CompilerParams(vmem_limit_bytes=VMEM_LIMIT),
        cost_estimate=pl.CostEstimate(
            flops=2 * rows * units * share * len(masks),
            bytes_accessed=2 * units * share * len(masks), transcendentals=0,
        ),
        name="keep_down",
    )(place, h, *hbm(wd))


def project_kernel(*refs):
    out_ref = refs[-1]
    count = (len(refs) - 1) // 2
    total = None
    for x, w in zip(refs[:count], refs[count:-1]):
        p = mm(x[...], w[...]).astype(bf16).astype(f32)
        total = p if total is None else total + p
    out_ref[...] = total.astype(bf16)


def project(xs, ws):
    rows, lanes = xs[0].shape
    width = ws[0].shape[1]
    tile = tile_of(width, 512)
    return pl.pallas_call(
        project_kernel,
        grid=(width // tile,),
        in_specs=[pl.BlockSpec((rows, lanes), lambda i: (0, 0))] * len(xs)
        + [pl.BlockSpec((lanes, tile), lambda i: (0, i))] * len(ws),
        out_specs=pl.BlockSpec((rows, tile), lambda i: (0, i)),
        out_shape=jax.ShapeDtypeStruct((rows, width), bf16),
        compiler_params=pltpu.CompilerParams(vmem_limit_bytes=VMEM_LIMIT),
        cost_estimate=pl.CostEstimate(
            flops=2 * rows * lanes * width * len(xs),
            bytes_accessed=2 * lanes * width * len(xs), transcendentals=0,
        ),
        name="project",
    )(*xs, *ws)


def swap(x, mask):
    count = lax.axis_size("tp")
    return lax.ppermute(x, "tp", [(i, i ^ mask) for i in range(count)])


def hop(x, mask):
    count = lax.axis_size("ep")
    return lax.ppermute(x, "ep", [(i, i ^ mask) for i in range(count)])


def gathered(x, far=None):
    masks, blocks = [0], [x]
    mask = lax.axis_size("tp") // 2
    if far is not None:
        masks, blocks, mask = [0, mask], [x, far], mask // 2
    while mask:
        more = []
        for b in blocks:
            more.append(swap(b, mask))
        blocks += more
        masks += [m ^ mask for m in masks]
        mask //= 2
    return tuple(masks), blocks


def local(
    receptance, key_matrix, value_matrix, decay_data_term, correction_rate_data,
    output_gate_input, decay_channel_offset, correction_rate_offset, extra_head_log_decay,
    head_norm_gain, mixer_output_weight, expert_layer_input, feedforward_norm_gain,
    group_router_weight, expert_router_weight, routes, expert_gate_weight, expert_up_weight,
    expert_down_weight,
):
    ep, tp = lax.axis_size("ep"), lax.axis_size("tp")
    place = lax.axis_index("tp").reshape(1).astype(jnp.int32)
    turn = lax.axis_index("ep").reshape(1).astype(jnp.int32)
    both = jnp.concatenate([place, turn])
    tokens, width = expert_layer_input.shape
    experts = expert_router_weight.shape[1]
    share = width // tp
    capacity = 4 * tokens // ep

    weight_far = swap(mixer_output_weight, tp // 2)
    send, info = route(
        place, expert_layer_input, feedforward_norm_gain, group_router_weight.T,
        expert_router_weight.T, routes.T, 1, capacity, share,
    )
    arrived = lax.all_to_all(send, "ep", split_axis=0, concat_axis=0, tiled=True)

    mixer_args = (
        receptance, key_matrix, value_matrix, decay_data_term, correction_rate_data,
        decay_channel_offset, correction_rate_offset, extra_head_log_decay.T,
    )
    local_a, reach_a, state = mixer_local(0, ep, None, *mixer_args)
    arrived, state = lax.optimization_barrier((arrived, state))
    rows_in = arrived.reshape(experts * capacity, share)
    far = swap(rows_in, tp // 2)
    local_b, reach_b, end = mixer_local(1, ep, state, *mixer_args)
    far, weight_far, local_b = lax.optimization_barrier((far, weight_far, local_b))
    weight_masks, weight_blocks = gathered(mixer_output_weight, weight_far)
    ends = lax.all_to_all(end, "ep", split_axis=0, concat_axis=0, tiled=True)

    masks, blocks = gathered(rows_in, far)
    odd = [m for m in range(tp) if m & 1]
    even = [m for m in range(tp) if not m & 1]
    h, send = run_experts(
        both, masks, odd, blocks, expert_gate_weight, expert_up_weight, expert_down_weight, ep
    )
    keep = keep_down(place, even, h, expert_down_weight, share)
    bit = 1
    got = swap(send, bit)
    while 2 * bit < tp:
        bit *= 2
        if 2 * bit < tp:
            keep, send = split(keep, got, 1)
            got = swap(send, bit)
        else:
            keep, near, away = split(keep, got, 2)
    half = near.shape[1]
    away = swap(away, bit)
    near = swap(near, bit)
    away = merge(keep, away, half, capacity)
    away = [hop(x, ep // 2 + m) for m, x in enumerate(away)]
    near = merge(keep, near, 0, capacity)
    near = [near[0]] + [hop(x, m) for m, x in enumerate(near) if m]
    homes = near + away

    mixed = mixer_finish(
        both, ends, output_gate_input, head_norm_gain,
        (local_a, local_b), (reach_a, reach_b), tp,
    )
    pieces = [mixed[m] if m == 0 else swap(mixed[m], m) for m in weight_masks]
    token_mixer_output = project(pieces, weight_blocks)
    expert_out = combine(both, info, homes, routes.shape[1])
    return (token_mixer_output, expert_out)


def solution(mesh):
    in_specs = (
        P("ep", "tp"), P("ep", "tp"), P("ep", "tp"), P("ep", "tp"), P("ep", "tp"), P("ep", "tp"),
        P("tp"), P("tp"), P("ep", "tp"), P("tp"), P("tp", None), P("ep", None), P(), P(), P(),
        P("ep", None), P("ep", None, "tp"), P("ep", None, "tp"), P("ep", "tp", None),
    )
    out_specs = (P(("ep", "tp"), None), P("ep", "tp"))
    return jax.shard_map(local, mesh=mesh, in_specs=in_specs, out_specs=out_specs, check_vma=False)
```
